32 devices in a mesh: fs: 8 (over z, y), tp: 4 (over x, core).
Axes of the slice: x: 2, y: 2, z: 4, core: 2. Of those that a mesh axis runs over, the one named last changes fastest.
Arguments:
- tokens: bfloat16 [6144, 2048], P('fs'), may hold values from -6 to 6
- norm_gain: float32 [2048], P('fs'), may hold values from 0.1 to 1.9
- gate_weight: float32 [2048, 5632], P('fs', 'tp'), may hold values from -0.125 to 0.125
- up_weight: float32 [2048, 5632], P('fs', 'tp'), may hold values from -0.125 to 0.125
- down_weight: float32 [5632, 2048], P('fs', 'tp'), may hold values from -0.078125 to 0.078125
Outputs:
- gate_out: bfloat16 [2048, 5632], P(None, 'tp')
- up_out: bfloat16 [2048, 5632], P(None, 'tp')
- down_out: bfloat16 [5632, 2048], P('tp')
- mixed: bfloat16 [6144, 2048], P('fs', 'tp')
The draws below stay inside these ranges and needn't reach their ends.
All inputs are finite; a program needn't handle non-finite values.
Results may differ from the reference program's by a relative error of at most 0.0095.
Values may be sent and summed in bfloat16 or wider, within the bound.
A program may use at most 128 MiB of HBM per device.

```python
import jax
import jax.numpy as jnp
from jax import lax

D = 2048
FF = 5632
TOKENS = 6144
N_TP = 4


def level_of(stream_key, dims, cuts, least, largest):
    gain, own = 1.0, jax.random.fold_in(stream_key, 6)
    for dim, blocks in cuts:
        heights = jnp.exp(jax.random.uniform(jax.random.fold_in(own, dim), (blocks,), jnp.float32, least / len(cuts), largest / len(cuts)))
        gain = gain * jnp.repeat(heights, dims[dim] // blocks).reshape([-1 if axis == dim else 1 for axis in range(len(dims))])
    return gain


def centred(rng, dims, width, reach, cuts=(), kind=jnp.bfloat16):
    result = width * jax.random.normal(rng, dims, jnp.float32)
    if cuts:
        result = result * level_of(rng, dims, cuts, -0.22, 0.18)
    return jnp.clip(result, -reach, reach).astype(kind)


def setup_inputs(seed: int = 0) -> dict:
    splits = jax.random.split(jax.random.key(seed), 6)
    return {
        "tokens": centred(splits[0], (TOKENS, D), 1.0, 6.0, ((0, 8),)),
        "norm_gain": jnp.clip(1.0 + 0.18 * jax.random.normal(splits[1], (D,), jnp.float32), 0.1, 1.9),
        "gate_weight": centred(splits[2], (D, FF), D ** -0.5, 0.125, ((0, 8), (1, 4)), jnp.float32),
        "up_weight": centred(splits[3], (D, FF), D ** -0.5, 0.125, ((0, 8), (1, 4)), jnp.float32),
        "down_weight": centred(splits[4], (FF, D), FF ** -0.5, 0.078125, ((0, 8), (1, 4)), jnp.float32),
    }


eps_norm = 1e-06

def reference(tokens, norm_gain, gate_weight, up_weight, down_weight):
    gain_column = norm_gain[:, None]
    gate_out = (gate_weight * gain_column).astype(jnp.bfloat16)
    up_out = (up_weight * gain_column).astype(jnp.bfloat16)
    down_out = down_weight.astype(jnp.bfloat16)
    rows_float = tokens.astype(jnp.float32)
    normed = (rows_float * lax.rsqrt(lax.optimization_barrier(jnp.mean(rows_float * rows_float, axis=-1, keepdims=True)) + eps_norm)).astype(jnp.bfloat16)
    gate_act = jnp.dot(normed, gate_out, preferred_element_type=jnp.float32)
    up_act = jnp.dot(normed, up_out, preferred_element_type=jnp.float32)
    hidden = (jax.nn.silu(gate_act) * up_act).astype(jnp.bfloat16)
    block_rows = FF // N_TP
    total = jnp.zeros((tokens.shape[0], D), jnp.float32)
    for index in range(N_TP):
        lower = index * block_rows
        share = jnp.dot(hidden[:, lower:lower + block_rows], down_out[lower:lower + block_rows, :], preferred_element_type=jnp.float32).astype(jnp.bfloat16)
        total = total + share.astype(jnp.float32)
    mixed = total.astype(jnp.bfloat16)
    return (gate_out, up_out, down_out, mixed)
```

```python
import functools
import heapq

import jax
import jax.numpy as jnp
from jax import lax
from jax.experimental import pallas as pl
from jax.experimental.pallas import tpu as pltpu
from jax.sharding import PartitionSpec as P

eps_norm = 1e-06
MESH = pl.DeviceIdType.MESH

PIECES = (
    ("gate", 0, 1, "a"),
    ("gate", 1, 1, "a"),
    ("down", 2, 2, "b"),
    ("up", 0, 1, "a"),
    ("up", 1, 1, "a"),
    ("down", 0, 1, "a"),
    ("down", 1, 1, "a"),
)
PHASES = ((0, 1, 6), (2,), (3, 4), (5,))
GROUPS = ((1, 3, (2, 6)), (0, 1, (5,)))


def cost(p):
    return 0.5 if PIECES[p][0] == "down" and kind(p) == 1 else 1.0


def kind(p):
    return PIECES[p][3]


def plan(n_z):
    events = []
    seq = [(d, p) for phase in PHASES for d in range(1, n_z) for p in phase]
    order = sorted(range(len(PIECES)), key=lambda p: kind(p) == "a")
    own, total = {}, 0.0
    for p in order:
        total += cost(p)
        own[p] = total
    z_time, now = {}, 0.0
    for i, phase in enumerate(PHASES):
        for d in range(1, n_z):
            if d == n_z - 1 and i + 1 < len(PHASES):
                events.append((now + 0.02, 1, "launch", i + 1, 0))
            for p in phase:
                if kind(p) == "a":
                    now += cost(p)
                    z_time[d, p] = now
                    events.append((now, 0, "line", d, p))
                else:
                    now += 2.0 * cost(p)
                    z_time[d, p] = now
                    events.append((now - cost(p), 0, "line", d, p))
                    events.append((now, 0, "line_other", d, p))
    y_time = {}
    for z in range(n_z):
        at = total
        for d, p in seq:
            if kind(p) == "a":
                for zz in (z - d, z + d):
                    if 0 <= zz < n_z:
                        at = max(at, z_time[d, p]) + cost(p)
                        y_time[d, p] = max(y_time.get((d, p), 0.0), at)
    for p, at in own.items():
        events.append((at, 1, "pair", 0, p))
    for (d, p), at in y_time.items():
        events.append((at, 1, "pair", d, p))
    here = dict(y_time)
    here.update({(0, p): at for p, at in own.items()})
    last = 0.0
    for name in ("gate", "up"):
        mine = [p for p in range(len(PIECES)) if PIECES[p][0] == name]
        for d in range(n_z):
            at = max(here[d, p] for p in mine) + 0.01
            events.append((at, 2, "mul_" + name, d, 0))
            last = max(last, at)
    events.append((last + 0.01, 3, "act", 0, 0))
    end = max(e[0] for e in events) + 0.1
    for step in range(4):
        events.append((end + 0.01 + 0.01 * step, 4, "share", 0, step))
    for step in range(5):
        events.append((end + 0.1 + 0.1 * step, 4, "share", 1, step))
    events.append((end + 0.35, 4, "share", 0, 4))
    return sorted(events)


def kernel(
    n_fs, n_tp, tok_hbm, gain, gw, uw, dw, gate_o, up_o, down_o, mix_o,
    tok, dcol, normed, acc_g, acc_u, hidden, share0, share1, pair0, pair1, send0, send1, in0, in1,
    tok_sem, ag_send, ag_recv, aa_send, aa_recv, rs_send, rs_recv,
):
    tok_copy = pltpu.make_async_copy(tok_hbm, tok, tok_sem)
    tok_copy.start()
    shares, pairs, sends, ins = (share0, share1), (pair0, pair1), (send0, send1), (in0, in1)
    f, t = lax.axis_index("fs"), lax.axis_index("tp")
    n_z = n_fs // 2
    z, y = f // 2, f % 2
    per = n_fs // n_tp
    rows = gw.shape[0]
    d_rows, d_cols = dw.shape
    part = d_cols // 4
    n_tok = tok.shape[0]
    k_z = normed.shape[2]
    m_tile = min(256, n_tok)
    width = gw.shape[1]
    col_tiles = [(c, min(512, width - c)) for c in range(0, width, 512)]

    def flip(bit):
        return t + bit - 2 * bit * ((t // bit) % 2)

    near, far = flip(1), flip(2)
    far_near = far + 1 - 2 * (far % 2)

    def view(o, p):
        name, h, n, _ = PIECES[p]
        if name == "down":
            return dcol.at[o, :, pl.ds(h * part, n * part)]
        ref = gate_o if name == "gate" else up_o
        return ref.at[pl.ds(pl.multiple_of(o * rows + h * (rows // 2), rows // 2), rows // 2), :]

    def ag(o, p, way, dest):
        v = view(o, p)
        return pltpu.make_async_remote_copy(
            v, v, ag_send.at[o, p, way], ag_recv.at[o, p],
            device_id=(dest, t), device_id_type=MESH,
        )

    started = []

    def start(cond, make):
        if cond is None:
            make().start()
        else:
            pl.when(cond)(lambda: make().start())
        started.append((cond, make))

    def land(o, p):
        ag(o, p, 0, f).wait_recv()

    def exchange(cond, o, p):
        name, h, n, _ = PIECES[p]
        if name != "down":
            return
        owner = o // per
        k = o % per
        row = pl.multiple_of(k * d_rows, d_rows)
        col = pl.multiple_of(t * d_cols + h * part, part)

        def make():
            return pltpu.make_async_remote_copy(
                view(o, p), down_o.at[pl.ds(row, d_rows), pl.ds(col, n * part)],
                aa_send.at[o, p], aa_recv.at[t, k, p],
                device_id=(f, owner), device_id_type=MESH,
            )

        away = owner != t
        start(away if cond is None else jnp.logical_and(cond, away), make)
        mine = owner == t

        @pl.when(mine if cond is None else jnp.logical_and(cond, mine))
        def _():
            down_o[pl.ds(row, d_rows), pl.ds(col, n * part)] = dcol[o, :, h * part : (h + n) * part]

    barrier = pltpu.get_barrier_semaphore()
    other_y = f + 1 - 2 * y
    peers = [
        (z > 0, (f - 2, t)), (z < n_z - 1, (f + 2, t)), (None, (other_y, t)),
        (None, (f, near)), (None, (f, far)), (None, (f, far_near)),
    ]
    for cond, dev in peers:
        def hello(dev=dev):
            pl.semaphore_signal(barrier, inc=1, device_id=dev, device_id_type=MESH)
        hello() if cond is None else pl.when(cond)(hello)

    g = jnp.broadcast_to(gain[...], (8, rows)).T[:, :1]
    base = pl.multiple_of(f * rows, rows)
    gate_o[pl.ds(base, rows), :] = (gw[...] * g).astype(jnp.bfloat16)
    dcol[f] = dw[...].astype(jnp.bfloat16)
    up_o[pl.ds(base, rows), :] = (uw[...] * g).astype(jnp.bfloat16)
    inner = jnp.logical_and(z > 0, z < n_z - 1)
    pl.when(inner)(lambda: pl.semaphore_wait(barrier, len(peers)))
    pl.when(jnp.logical_not(inner))(lambda: pl.semaphore_wait(barrier, len(peers) - 1))

    def launch(phase):
        for p in PHASES[phase]:
            start(z > 0, functools.partial(ag, f, p, 0, f - 2))
            start(z < n_z - 1, functools.partial(ag, f, p, 1, f + 2))
            if kind(p) == "b":
                other_b(p)

    def other_b(p):
        start(z > 0, functools.partial(ag, other_y, p, 0, f - 2))
        start(z < n_z - 1, functools.partial(ag, other_y, p, 1, f + 2))

    for p in sorted(range(len(PIECES)), key=lambda p: kind(p) == "a"):
        start(None, functools.partial(ag, f, p, 2, other_y))
    for p in PHASES[0]:
        start(z > 0, functools.partial(ag, f, p, 0, f - 2))
        start(z < n_z - 1, functools.partial(ag, f, p, 1, f + 2))
    for p in range(len(PIECES)):
        exchange(None, f, p)

    n_norm = n_tok // 64
    tok_copy.wait()

    @pl.loop(0, n_norm)
    def _(i):
        r = pl.multiple_of(i * 64, 64)
        x = tok[pl.ds(r, 64), :].astype(jnp.float32)
        x = x * lax.rsqrt(jnp.mean(x * x, axis=-1, keepdims=True) + eps_norm)
        x = x.astype(jnp.bfloat16)
        for j in range(n_z):
            normed[j, pl.ds(r, 64), :] = x[:, j * k_z : (j + 1) * k_z]

    def multiply(w, acc, zz, first):
        k0 = pl.multiple_of(zz * k_z, k_z)

        @pl.loop(0, n_tok // m_tile)
        def _(i):
            r = pl.multiple_of(i * m_tile, m_tile)
            a = normed[zz, pl.ds(r, m_tile), :]
            for c, n in col_tiles:
                v = jnp.dot(a, w[pl.ds(k0, k_z), c : c + n], preferred_element_type=jnp.float32)
                if first:
                    acc[pl.ds(r, m_tile), c : c + n] = v
                else:
                    acc[pl.ds(r, m_tile), c : c + n] += v

    def sides(d):
        return [(z >= d, z - d, -1), (z + d < n_z, z + d, 1)]

    def forward(cond, zz, sign, o, p):
        if sign < 0:
            start(jnp.logical_and(cond, z < n_z - 1), functools.partial(ag, o, p, 1, f + 2))
        else:
            start(jnp.logical_and(cond, z > 0), functools.partial(ag, o, p, 0, f - 2))

    def share_step(group, step):
        q, n, parts = GROUPS[group]
        share, half_in, out_send, out_in = shares[group], pairs[group], sends[group], ins[group]
        wide = n * part

        def aa_wait(c):
            for k in range(per):
                for p in parts:
                    _, h, m, _ = PIECES[p]
                    ref = down_o.at[
                        pl.ds(k * d_rows, d_rows), pl.ds(pl.multiple_of(c * d_cols + h * part, part), m * part)
                    ]
                    pltpu.make_async_remote_copy(
                        ref, ref, aa_send.at[0, p], aa_recv.at[c, k, p], device_id=(f, near), device_id_type=MESH,
                    ).wait_recv()

        def product(c, slot):
            @pl.loop(0, n_tok // m_tile)
            def _(i):
                r = pl.multiple_of(i * m_tile, m_tile)
                col = pl.multiple_of(c * d_cols + q * part, part)
                v = jnp.dot(hidden[pl.ds(r, m_tile), :], down_o[:, pl.ds(col, wide)], preferred_element_type=jnp.float32)
                share[slot, pl.ds(r, m_tile), :] = v.astype(jnp.bfloat16)

        def pair(slot):
            return pltpu.make_async_remote_copy(
                share.at[slot], half_in.at[slot], rs_send.at[group, slot], rs_recv.at[group, slot],
                device_id=(f, near), device_id_type=MESH,
            )

        def across():
            return pltpu.make_async_remote_copy(
                out_send, out_in, rs_send.at[group, 2], rs_recv.at[group, 2],
                device_id=(f, far), device_id_type=MESH,
            )

        if step == 0:
            aa_wait(far_near)
            product(far_near, 0)
            start(None, functools.partial(pair, 0))
        elif step == 1:
            aa_wait(far)
            product(far, 2)
            pair(0).wait_recv()
            out_send[...] = (share[2].astype(jnp.float32) + half_in[0].astype(jnp.float32)).astype(jnp.bfloat16)
            start(None, across)
        elif step == 2:
            aa_wait(near)
            product(near, 1)
            start(None, functools.partial(pair, 1))
        elif step == 3:
            product(t, 3)
        elif step == 4:
            pair(1).wait_recv()
            across().wait_recv()
            mix_o[:, q * part : (q + n) * part] = (
                share[3].astype(jnp.float32) + half_in[1].astype(jnp.float32) + out_in[...].astype(jnp.float32)
            ).astype(jnp.bfloat16)

    for _, _, what, d, p in plan(n_z):
        if what == "launch":
            launch(d)
        elif what == "share":
            share_step(d, p)
        elif what == "line":
            for cond, zz, sign in sides(d):
                o = zz * 2 + y
                pl.when(cond)(functools.partial(land, o, p))
                forward(cond, zz, sign, o, p)
                if kind(p) == "a":
                    start(cond, functools.partial(ag, o, p, 2, other_y))
                exchange(cond, o, p)
        elif what == "line_other":
            for cond, zz, sign in sides(d):
                o = zz * 2 + 1 - y
                pl.when(cond)(functools.partial(land, o, p))
                forward(cond, zz, sign, o, p)
                exchange(cond, o, p)
        elif what == "pair":
            if d == 0:
                land(other_y, p)
                exchange(None, other_y, p)
            else:
                for cond, zz, sign in sides(d):
                    o = zz * 2 + 1 - y
                    pl.when(cond)(functools.partial(land, o, p))
                    exchange(cond, o, p)
        elif what == "mul_gate" or what == "mul_up":
            w, acc = (gate_o, acc_g) if what == "mul_gate" else (up_o, acc_u)
            if d == 0:
                multiply(w, acc, z, True)
            else:
                for cond, zz, sign in sides(d):
                    pl.when(cond)(functools.partial(multiply, w, acc, zz, False))
        elif what == "act":
            @pl.loop(0, n_tok // 32)
            def _(i):
                r = pl.multiple_of(i * 32, 32)
                v = acc_g[pl.ds(r, 32), :]
                hidden[pl.ds(r, 32), :] = (v / (1.0 + jnp.exp(-v)) * acc_u[pl.ds(r, 32), :]).astype(jnp.bfloat16)

    for cond, make in started:
        if cond is None:
            make().wait_send()
        else:
            pl.when(cond)(lambda make=make: make().wait_send())


def on_device(n_fs, n_tp, tokens, norm_gain, gate_weight, up_weight, down_weight):
    n_tok, d_model = tokens.shape
    rows, width = gate_weight.shape
    d_rows, d_cols = down_weight.shape
    part = d_cols // 4
    n_z = n_fs // 2
    n_p = len(PIECES)
    bf = jnp.bfloat16
    vmem = pl.BlockSpec(memory_space=pltpu.VMEM)
    dma = pltpu.SemaphoreType.DMA
    return pl.pallas_call(
        functools.partial(kernel, n_fs, n_tp),
        out_shape=(
            pltpu.VMEM((d_model, width), bf),
            pltpu.VMEM((d_model, width), bf),
            pltpu.VMEM((d_rows * n_fs // n_tp, d_model), bf),
            pltpu.VMEM((n_tok, d_cols), bf),
        ),
        in_specs=[pl.BlockSpec(memory_space=pl.ANY)] + [vmem] * 4,
        out_specs=(vmem,) * 4,
        scratch_shapes=[
            pltpu.VMEM((n_tok, d_model), bf),
            pltpu.VMEM((n_fs, d_rows, d_cols), bf),
            pltpu.VMEM((n_z, n_tok, d_model // n_z), bf),
            pltpu.VMEM((n_tok, width), jnp.float32),
            pltpu.VMEM((n_tok, width), jnp.float32),
            pltpu.VMEM((n_tok, width), bf),
            *[pltpu.VMEM((4, n_tok, g[1] * part), bf) for g in GROUPS],
            *[pltpu.VMEM((2, n_tok, g[1] * part), bf) for g in GROUPS],
            *[pltpu.VMEM((n_tok, g[1] * part), bf) for g in GROUPS],
            *[pltpu.VMEM((n_tok, g[1] * part), bf) for g in GROUPS],
            dma,
            dma((n_fs, n_p, 3)),
            dma((n_fs, n_p)),
            dma((n_fs, n_p)),
            dma((n_tp, n_fs // n_tp, n_p)),
            dma((2, 3)),
            dma((2, 3)),
        ],
        compiler_params=pltpu.CompilerParams(
            collective_id=0, has_side_effects=True, vmem_limit_bytes=46 * 2**20
        ),
    )(tokens, norm_gain[None, :], gate_weight, up_weight, down_weight)


PARTS = (
    ("gate", 0, 8, "a"),
    ("gate", 8, 8, "a"),
    ("up", 0, 6, "a"),
    ("up", 6, 5, "a"),
    ("up", 11, 5, "b"),
    ("down", 0, 1, "a"),
    ("down", 1, 1, "a"),
    ("down", 2, 1, "a"),
    ("down", 3, 1, "b"),
)
DOWN = tuple(p for p in range(len(PARTS)) if PARTS[p][0] == "down")
FAR_GROUPS = ((0, 2), (2, 2))
NEAR_GROUPS = ((0, 2), (2, 1), (3, 1))
UNIT, LAG, LEAD = 7.73, 2.0, 16.0


def crossing(src, p, n_z):
    return PARTS[p][0] == "down" and 2 * src >= n_z


def sort_of(src, p, n_z):
    return "a" if crossing(src, p, n_z) else PARTS[p][3]


def length(p):
    return UNIT * (0.5 if PARTS[p][0] == "down" else PARTS[p][2] / 8)


def rank(n_z, m, link, item):
    src, side, p = item
    if link == "x":
        return (0,)
    b = sort_of(src, p, n_z) == "b"
    if link == "y" and b:
        return (0, p)
    if PARTS[p][0] == "down":
        return (1 if crossing(src, p, n_z) else 4, p, abs(src - m), side)
    return (3 if b else 2, p, abs(src - m), side)


def simulate(n_z):
    queue, free, sent = {}, {}, {}
    events, have = [], [{} for _ in range(n_z)]
    far_in = [{} for _ in range(n_z)]
    count = [0]
    for m in range(n_z):
        for link in ("up", "dn", "y", "x"):
            queue[m, link], free[m, link], sent[m, link] = [], True, []

    def add(at, what, *rest):
        count[0] += 1
        heapq.heappush(events, (at, count[0], what, rest))

    def kick(at, m, link):
        if free[m, link] and queue[m, link]:
            queue[m, link].sort()
            _, item = queue[m, link].pop(0)
            free[m, link] = False
            sent[m, link].append((at, item))
            add(at + length(item[2]), "free", m, link)
            add(at + length(item[2]) + LAG, "land", m, link, item)

    def put(at, m, link, item):
        queue[m, link].append((rank(n_z, m, link, item), item))
        kick(at, m, link)

    def got(at, m, item):
        src, side, p = item
        have[m][item] = at
        b = sort_of(src, p, n_z) == "b"
        if side == 0 or b:
            if m >= src and m < n_z - 1:
                put(at, m, "up", item)
            if m <= src and m > 0:
                put(at, m, "dn", item)
        if side == 0 and (not b or m == src):
            put(at, m, "y", item)
        if crossing(src, p, n_z):
            put(at, m, "x", item)

    for m in range(n_z):
        for p in range(len(PARTS)):
            add(0.0, "own", m, (m, 0, p))
    while events:
        at, _, what, rest = heapq.heappop(events)
        if what == "own":
            got(at, *rest)
        elif what == "free":
            free[rest] = True
            kick(at, *rest)
        else:
            m, link, item = rest
            if link == "x":
                far_in[n_z - 1 - m][item] = at
            elif link == "y":
                got(at, m, (item[0], 1, item[2]))
            else:
                got(at, m + (1 if link == "up" else -1), item)
    return have, far_in, sent


def timetable(n_z):
    have, far_in, sent = simulate(n_z)
    sources, ready = {}, {}
    for m in range(n_z):
        for name in ("gate", "up"):
            mine = [p for p in range(len(PARTS)) if PARTS[p][0] == name]
            done = sorted((max(have[m][src, side, p] for side in (0, 1) for p in mine), src) for src in range(n_z))
            for j, (at, src) in enumerate(done):
                sources[m, name, j], ready[m, (name, j)] = src, at
        ready[m, ("norm", 0)] = 1.0
        ready[m, ("act", 0)] = 0.0
        for g, (q, n) in enumerate(FAR_GROUPS):
            ready[m, ("far", g)] = max(at for item, at in far_in[m].items() if q <= PARTS[item[2]][1] < q + n)
        for g, (q, n) in enumerate(NEAR_GROUPS):
            ready[m, ("near", g)] = 2.0 + max(
                at for item, at in have[m].items()
                if PARTS[item[2]][0] == "down" and not crossing(item[0], item[2], n_z) and q <= PARTS[item[2]][1] < q + n
            )
        ready[m, ("end", 0)] = 1e9
    muls = sorted(
        (sum(ready[m, (name, j)] for m in range(n_z)), name, j) for name in ("gate", "up") for j in range(n_z)
    )
    steps = [("norm", 0)] + [(name, j) for _, name, j in muls] + [("act", 0)]
    steps += [("far", g) for g in range(len(FAR_GROUPS))] + [("near", g) for g in range(len(NEAR_GROUPS))] + [("end", 0)]
    spans = {"norm": 3.0, "gate": 1.5, "up": 1.5, "act": 1.5, "far": 3.0, "near": 1.0, "end": 0.0}
    before = {}
    for m in range(n_z):
        todo = [(at, 0, "wait", item) for item, at in have[m].items() if at > 0.0]
        for link in ("up", "dn", "y", "x"):
            last = 0.0
            for at, item in sent[m, link]:
                last = max(last, have[m][item], at - LEAD)
                todo.append((last, 1, link, item))
        for item, at in have[m].items():
            if PARTS[item[2]][0] == "down" and not crossing(item[0], item[2], n_z):
                todo.append((at, 1, "core", item))
        todo.sort(key=lambda e: e[:2])
        now = 0.0
        for step in steps:
            now = max(now, ready[m, step])
            before[m, step] = [e[2:] for e in todo if e[0] <= now]
            todo = [e for e in todo if e[0] > now]
            now += spans[step[0]]
    return steps, sources, before


def line_kernel(
    n_fs, n_tp, tok_hbm, gain, gw, uw, dw, gate_o, up_o, down_o, mix_o,
    tok, dcol, normed, acc_g, acc_u, hidden, far_a, far_b, far_in, out_send, out_in, near_sh, near_in, own_sh,
    tok_sem, ag_send, ag_recv, aa_send, aa_recv, fp_send, fp_recv, ac_send, ac_recv, np_send, np_recv,
):
    tok_copy = pltpu.make_async_copy(tok_hbm, tok, tok_sem)
    tok_copy.start()
    f, t = lax.axis_index("fs"), lax.axis_index("tp")
    n_z = n_fs // 2
    z, y = f // 2, f % 2
    x = t // 2
    per = n_fs // n_tp
    rows = gw.shape[0]
    d_rows, d_cols = dw.shape
    part = d_cols // 4
    n_tok = tok.shape[0]
    k_z = normed.shape[2]
    m_tile = min(256, n_tok)
    width = gw.shape[1]
    col_tiles = [(c, min(512, width - c)) for c in range(0, width, 512)]
    place = z + x * (n_z - 1 - 2 * z)
    ahead = f + 2 - 4 * x
    behind = f - 2 + 4 * x
    other_y = f + 1 - 2 * y
    near = t + 1 - 2 * (t % 2)
    far = t + 2 - 4 * x
    far_near = far + 1 - 2 * (far % 2)
    steps, sources, before = timetable(n_z)

    def z_of(src):
        return src + x * (n_z - 1 - 2 * src)

    def owner_of(item):
        src, side, _ = item
        return 2 * z_of(src) + (y if side == 0 else 1 - y)

    def view(o, p):
        name, first, n, _ = PARTS[p]
        if name == "down":
            return dcol.at[o, :, pl.ds(first * part, n * part)]
        ref = gate_o if name == "gate" else up_o
        step = rows // 16
        return ref.at[pl.ds(pl.multiple_of(o * rows + first * step, step), n * step), :]

    def ag(item, way, dest):
        o, p = owner_of(item), item[2]
        v = view(o, p)
        return pltpu.make_async_remote_copy(
            v, v, ag_send.at[o, p, way], ag_recv.at[o, p], device_id=(dest, t), device_id_type=MESH,
        )

    def hand(item):
        o, p = owner_of(item), item[2]
        _, first, n, _ = PARTS[p]
        row = pl.multiple_of((o % per) * d_rows, d_rows)
        col = pl.multiple_of(t * d_cols + first * part, part)
        return pltpu.make_async_remote_copy(
            view(o, p), down_o.at[pl.ds(row, d_rows), pl.ds(col, n * part)],
            aa_send.at[o, p], aa_recv.at[t, o % per, p],
            device_id=(f, o // per), device_id_type=MESH,
        )

    def transfer(what, item):
        if what == "up":
            return ag(item, 0, ahead)
        if what == "dn":
            return ag(item, 1, behind)
        if what == "y":
            return ag(item, 2, other_y)
        return hand(item)

    def elsewhere(item):
        return owner_of(item) // per != t

    def play(step):
        for m in range(n_z):
            def events(m=m):
                for what, item in before[m, step]:
                    if what == "wait":
                        ag(item, 0, f).wait_recv()
                    elif what == "core":
                        pl.when(elsewhere(item))(lambda item=item: hand(item).start())
                    else:
                        transfer(what, item).start()
            if before[m, step]:
                pl.when(place == m)(events)

    barrier = pltpu.get_barrier_semaphore()
    peers = [
        (z > 0, (f - 2, t)), (z < n_z - 1, (f + 2, t)), (None, (other_y, t)),
        (None, (f, near)), (None, (f, far)), (None, (f, far_near)),
    ]
    for cond, dev in peers:
        def hello(dev=dev):
            pl.semaphore_signal(barrier, inc=1, device_id=dev, device_id_type=MESH)
        hello() if cond is None else pl.when(cond)(hello)

    g = jnp.broadcast_to(gain[...], (8, rows)).T[:, :1]
    base = pl.multiple_of(f * rows, rows)
    gate_o[pl.ds(base, rows), :] = (gw[...] * g).astype(jnp.bfloat16)
    dcol[f] = dw[...].astype(jnp.bfloat16)
    up_o[pl.ds(base, rows), :] = (uw[...] * g).astype(jnp.bfloat16)
    inner = jnp.logical_and(z > 0, z < n_z - 1)
    pl.when(inner)(lambda: pl.semaphore_wait(barrier, len(peers)))
    pl.when(jnp.logical_not(inner))(lambda: pl.semaphore_wait(barrier, len(peers) - 1))

    def norm():
        tok_copy.wait()

        @pl.loop(0, n_tok // 64)
        def _(i):
            r = pl.multiple_of(i * 64, 64)
            v = tok[pl.ds(r, 64), :].astype(jnp.float32)
            v = v * lax.rsqrt(jnp.mean(v * v, axis=-1, keepdims=True) + eps_norm)
            v = v.astype(jnp.bfloat16)
            for j in range(n_z):
                normed[j, pl.ds(r, 64), :] = v[:, j * k_z : (j + 1) * k_z]

    def multiply(w, acc, src, first):
        zz = z_of(src)
        k0 = pl.multiple_of(zz * k_z, k_z)

        @pl.loop(0, n_tok // m_tile)
        def _(i):
            r = pl.multiple_of(i * m_tile, m_tile)
            a = normed[zz, pl.ds(r, m_tile), :]
            for c, n in col_tiles:
                v = jnp.dot(a, w[pl.ds(k0, k_z), c : c + n], preferred_element_type=jnp.float32)
                if first:
                    acc[pl.ds(r, m_tile), c : c + n] = v
                else:
                    acc[pl.ds(r, m_tile), c : c + n] += v

    def act():
        @pl.loop(0, n_tok // 32)
        def _(i):
            r = pl.multiple_of(i * 32, 32)
            v = acc_g[pl.ds(r, 32), :]
            hidden[pl.ds(r, 32), :] = (v / (1.0 + jnp.exp(-v)) * acc_u[pl.ds(r, 32), :]).astype(jnp.bfloat16)

    def arrived(c, q, n):
        for k in range(per):
            for p in DOWN:
                _, first, m, _ = PARTS[p]
                if q <= first < q + n:
                    ref = down_o.at[
                        pl.ds(k * d_rows, d_rows), pl.ds(pl.multiple_of(c * d_cols + first * part, part), m * part)
                    ]
                    pltpu.make_async_remote_copy(
                        ref, ref, aa_send.at[0, p], aa_recv.at[c, k, p], device_id=(f, near), device_id_type=MESH,
                    ).wait_recv()

    def product(c, q, n, out):
        @pl.loop(0, n_tok // m_tile)
        def _(i):
            r = pl.multiple_of(i * m_tile, m_tile)
            col = pl.multiple_of(c * d_cols + q * part, part)
            v = jnp.dot(
                hidden[pl.ds(r, m_tile), :], down_o[:, pl.ds(col, n * part)], preferred_element_type=jnp.float32
            )
            out[pl.ds(r, m_tile), :] = v.astype(jnp.bfloat16)

    def cols(q, n):
        return slice(q * part, (q + n) * part)

    def far_pair(i):
        q, n = FAR_GROUPS[i]
        return pltpu.make_async_remote_copy(
            far_a.at[:, cols(q, n)], far_in.at[:, cols(q, n)], fp_send.at[i], fp_recv.at[i],
            device_id=(f, near), device_id_type=MESH,
        )

    def across(i):
        q, n = FAR_GROUPS[i]
        return pltpu.make_async_remote_copy(
            out_send.at[:, cols(q, n)], out_in.at[:, cols(q, n)], ac_send.at[i], ac_recv.at[i],
            device_id=(f, far), device_id_type=MESH,
        )

    def near_pair(i):
        q, n = NEAR_GROUPS[i]
        return pltpu.make_async_remote_copy(
            near_sh.at[:, cols(q, n)], near_in.at[:, cols(q, n)], np_send.at[i], np_recv.at[i],
            device_id=(f, near), device_id_type=MESH,
        )

    def far_step(i):
        q, n = FAR_GROUPS[i]
        arrived(far_near, q, n)
        product(far_near, q, n, far_a.at[:, cols(q, n)])
        far_pair(i).start()
        arrived(far, q, n)
        product(far, q, n, far_b.at[:, cols(q, n)])
        far_pair(i).wait_recv()
        out_send[:, cols(q, n)] = (
            far_b[:, cols(q, n)].astype(jnp.float32) + far_in[:, cols(q, n)].astype(jnp.float32)
        ).astype(jnp.bfloat16)
        across(i).start()

    def near_step(i):
        q, n = NEAR_GROUPS[i]
        col = pl.multiple_of(t * d_cols + q * part, part)
        for k in range(per):
            down_o[k * d_rows : (k + 1) * d_rows, pl.ds(col, n * part)] = dcol[t * per + k, :, cols(q, n)]
        arrived(near, q, n)
        product(near, q, n, near_sh.at[:, cols(q, n)])
        near_pair(i).start()
        product(t, q, n, own_sh.at[:, cols(q, n)])

    def end():
        for i in range(len(FAR_GROUPS)):
            across(i).wait_recv()
        for i, (q, n) in enumerate(NEAR_GROUPS):
            near_pair(i).wait_recv()
            c = cols(q, n)
            mix_o[:, c] = (
                own_sh[:, c].astype(jnp.float32) + near_in[:, c].astype(jnp.float32) + out_in[:, c].astype(jnp.float32)
            ).astype(jnp.bfloat16)

    done = {"gate": 0, "up": 0}
    for step in steps:
        play(step)
        what, i = step
        if what == "norm":
            norm()
        elif what == "act":
            act()
        elif what == "far":
            far_step(i)
        elif what == "near":
            near_step(i)
        elif what == "end":
            end()
        else:
            src = sources[0, what, i]
            for m in range(1, n_z):
                src = jnp.where(place == m, sources[m, what, i], src)
            multiply(gate_o if what == "gate" else up_o, acc_g if what == "gate" else acc_u, src, done[what] == 0)
            done[what] += 1

    for i in range(len(FAR_GROUPS)):
        far_pair(i).wait_send()
        across(i).wait_send()
    for i in range(len(NEAR_GROUPS)):
        near_pair(i).wait_send()
    for m in range(n_z):
        @pl.when(place == m)
        def _(m=m):
            for step in steps:
                for what, item in before[m, step]:
                    if what == "core":
                        pl.when(elsewhere(item))(lambda item=item: hand(item).wait_send())
                    elif what != "wait":
                        transfer(what, item).wait_send()


def line_on_device(n_fs, n_tp, tokens, norm_gain, gate_weight, up_weight, down_weight):
    n_tok, d_model = tokens.shape
    rows, width = gate_weight.shape
    d_rows, d_cols = down_weight.shape
    n_z = n_fs // 2
    n_p = len(PARTS)
    bf = jnp.bfloat16
    vmem = pl.BlockSpec(memory_space=pltpu.VMEM)
    dma = pltpu.SemaphoreType.DMA
    n_far, n_near = len(FAR_GROUPS), len(NEAR_GROUPS)
    return pl.pallas_call(
        functools.partial(line_kernel, n_fs, n_tp),
        out_shape=(
            pltpu.VMEM((d_model, width), bf),
            pltpu.VMEM((d_model, width), bf),
            pltpu.VMEM((d_rows * n_fs // n_tp, d_model), bf),
            pltpu.VMEM((n_tok, d_cols), bf),
        ),
        in_specs=[pl.BlockSpec(memory_space=pl.ANY)] + [vmem] * 4,
        out_specs=(vmem,) * 4,
        scratch_shapes=[
            pltpu.VMEM((n_tok, d_model), bf),
            pltpu.VMEM((n_fs, d_rows, d_cols), bf),
            pltpu.VMEM((n_z, n_tok, d_model // n_z), bf),
            pltpu.VMEM((n_tok, width), jnp.float32),
            pltpu.VMEM((n_tok, width), jnp.float32),
            pltpu.VMEM((n_tok, width), bf),
            *[pltpu.VMEM((n_tok, d_cols), bf)] * 8,
            dma,
            dma((n_fs, n_p, 3)),
            dma((n_fs, n_p)),
            dma((n_fs, n_p)),
            dma((n_tp, n_fs // n_tp, n_p)),
            dma((n_far,)),
            dma((n_far,)),
            dma((n_far,)),
            dma((n_far,)),
            dma((n_near,)),
            dma((n_near,)),
        ],
        compiler_params=pltpu.CompilerParams(
            collective_id=0, has_side_effects=True, vmem_limit_bytes=46 * 2**20
        ),
    )(tokens, norm_gain[None, :], gate_weight, up_weight, down_weight)


def solution(mesh):
    n_fs, n_tp = mesh.shape["fs"], mesh.shape["tp"]
    in_specs = (P("fs", None), P("fs"), P("fs", "tp"), P("fs", "tp"), P("fs", "tp"))
    out_specs = (P(None, "tp"), P(None, "tp"), P("tp", None), P("fs", "tp"))
    body = line_on_device if (n_fs, n_tp) == (8, 4) else on_device
    return jax.shard_map(
        functools.partial(body, n_fs, n_tp), mesh=mesh, in_specs=in_specs, out_specs=out_specs, check_vma=False
    )
```

```python
import functools
import heapq

import jax
import jax.numpy as jnp
from jax import lax
from jax.experimental import pallas as pl
from jax.experimental.pallas import tpu as pltpu
from jax.sharding import PartitionSpec as P

eps_norm = 1e-06
MESH = pl.DeviceIdType.MESH

PIECES = (
    ("gate", 0, 1, "a"),
    ("gate", 1, 1, "a"),
    ("down", 2, 2, "b"),
    ("up", 0, 1, "a"),
    ("up", 1, 1, "a"),
    ("down", 0, 1, "a"),
    ("down", 1, 1, "a"),
)
PHASES = ((0, 1, 6), (2,), (3, 4), (5,))
GROUPS = ((1, 3, (2, 6)), (0, 1, (5,)))


def cost(p):
    return 0.5 if PIECES[p][0] == "down" and kind(p) == 1 else 1.0


def kind(p):
    return PIECES[p][3]


def plan(n_z):
    events = []
    seq = [(d, p) for phase in PHASES for d in range(1, n_z) for p in phase]
    order = sorted(range(len(PIECES)), key=lambda p: kind(p) == "a")
    own, total = {}, 0.0
    for p in order:
        total += cost(p)
        own[p] = total
    z_time, now = {}, 0.0
    for i, phase in enumerate(PHASES):
        for d in range(1, n_z):
            if d == n_z - 1 and i + 1 < len(PHASES):
                events.append((now + 0.02, 1, "launch", i + 1, 0))
            for p in phase:
                if kind(p) == "a":
                    now += cost(p)
                    z_time[d, p] = now
                    events.append((now, 0, "line", d, p))
                else:
                    now += 2.0 * cost(p)
                    z_time[d, p] = now
                    events.append((now - cost(p), 0, "line", d, p))
                    events.append((now, 0, "line_other", d, p))
    y_time = {}
    for z in range(n_z):
        at = total
        for d, p in seq:
            if kind(p) == "a":
                for zz in (z - d, z + d):
                    if 0 <= zz < n_z:
                        at = max(at, z_time[d, p]) + cost(p)
                        y_time[d, p] = max(y_time.get((d, p), 0.0), at)
    for p, at in own.items():
        events.append((at, 1, "pair", 0, p))
    for (d, p), at in y_time.items():
        events.append((at, 1, "pair", d, p))
    here = dict(y_time)
    here.update({(0, p): at for p, at in own.items()})
    last = 0.0
    for name in ("gate", "up"):
        mine = [p for p in range(len(PIECES)) if PIECES[p][0] == name]
        for d in range(n_z):
            at = max(here[d, p] for p in mine) + 0.01
            events.append((at, 2, "mul_" + name, d, 0))
            last = max(last, at)
    events.append((last + 0.01, 3, "act", 0, 0))
    end = max(e[0] for e in events) + 0.1
    for step in range(4):
        events.append((end + 0.01 + 0.01 * step, 4, "share", 0, step))
    for step in range(5):
        events.append((end + 0.1 + 0.1 * step, 4, "share", 1, step))
    events.append((end + 0.35, 4, "share", 0, 4))
    return sorted(events)


def kernel(
    n_fs, n_tp, tok_hbm, gain, gw, uw, dw, gate_o, up_o, down_o, mix_o,
    tok, dcol, normed, acc_g, acc_u, hidden, share0, share1, pair0, pair1, send0, send1, in0, in1,
    tok_sem, ag_send, ag_recv, aa_send, aa_recv, rs_send, rs_recv,
):
    tok_copy = pltpu.make_async_copy(tok_hbm, tok, tok_sem)
    tok_copy.start()
    shares, pairs, sends, ins = (share0, share1), (pair0, pair1), (send0, send1), (in0, in1)
    f, t = lax.axis_index("fs"), lax.axis_index("tp")
    n_z = n_fs // 2
    z, y = f // 2, f % 2
    per = n_fs // n_tp
    rows = gw.shape[0]
    d_rows, d_cols = dw.shape
    part = d_cols // 4
    n_tok = tok.shape[0]
    k_z = normed.shape[2]
    m_tile = min(256, n_tok)
    width = gw.shape[1]
    col_tiles = [(c, min(512, width - c)) for c in range(0, width, 512)]

    def flip(bit):
        return t + bit - 2 * bit * ((t // bit) % 2)

    near, far = flip(1), flip(2)
    far_near = far + 1 - 2 * (far % 2)

    def view(o, p):
        name, h, n, _ = PIECES[p]
        if name == "down":
            return dcol.at[o, :, pl.ds(h * part, n * part)]
        ref = gate_o if name == "gate" else up_o
        return ref.at[pl.ds(pl.multiple_of(o * rows + h * (rows // 2), rows // 2), rows // 2), :]

    def ag(o, p, way, dest):
        v = view(o, p)
        return pltpu.make_async_remote_copy(
            v, v, ag_send.at[o, p, way], ag_recv.at[o, p],
            device_id=(dest, t), device_id_type=MESH,
        )

    started = []

    def start(cond, make):
        if cond is None:
            make().start()
        else:
            pl.when(cond)(lambda: make().start())
        started.append((cond, make))

    def land(o, p):
        ag(o, p, 0, f).wait_recv()

    def exchange(cond, o, p):
        name, h, n, _ = PIECES[p]
        if name != "down":
            return
        owner = o // per
        k = o % per
        row = pl.multiple_of(k * d_rows, d_rows)
        col = pl.multiple_of(t * d_cols + h * part, part)

        def make():
            return pltpu.make_async_remote_copy(
                view(o, p), down_o.at[pl.ds(row, d_rows), pl.ds(col, n * part)],
                aa_send.at[o, p], aa_recv.at[t, k, p],
                device_id=(f, owner), device_id_type=MESH,
            )

        away = owner != t
        start(away if cond is None else jnp.logical_and(cond, away), make)
        mine = owner == t

        @pl.when(mine if cond is None else jnp.logical_and(cond, mine))
        def _():
            down_o[pl.ds(row, d_rows), pl.ds(col, n * part)] = dcol[o, :, h * part : (h + n) * part]

    barrier = pltpu.get_barrier_semaphore()
    other_y = f + 1 - 2 * y
    peers = [
        (z > 0, (f - 2, t)), (z < n_z - 1, (f + 2, t)), (None, (other_y, t)),
        (None, (f, near)), (None, (f, far)), (None, (f, far_near)),
    ]
    for cond, dev in peers:
        def hello(dev=dev):
            pl.semaphore_signal(barrier, inc=1, device_id=dev, device_id_type=MESH)
        hello() if cond is None else pl.when(cond)(hello)

    g = jnp.broadcast_to(gain[...], (8, rows)).T[:, :1]
    base = pl.multiple_of(f * rows, rows)
    gate_o[pl.ds(base, rows), :] = (gw[...] * g).astype(jnp.bfloat16)
    dcol[f] = dw[...].astype(jnp.bfloat16)
    up_o[pl.ds(base, rows), :] = (uw[...] * g).astype(jnp.bfloat16)
    inner = jnp.logical_and(z > 0, z < n_z - 1)
    pl.when(inner)(lambda: pl.semaphore_wait(barrier, len(peers)))
    pl.when(jnp.logical_not(inner))(lambda: pl.semaphore_wait(barrier, len(peers) - 1))

    def launch(phase):
        for p in PHASES[phase]:
            start(z > 0, functools.partial(ag, f, p, 0, f - 2))
            start(z < n_z - 1, functools.partial(ag, f, p, 1, f + 2))
            if kind(p) == "b":
                other_b(p)

    def other_b(p):
        start(z > 0, functools.partial(ag, other_y, p, 0, f - 2))
        start(z < n_z - 1, functools.partial(ag, other_y, p, 1, f + 2))

    for p in sorted(range(len(PIECES)), key=lambda p: kind(p) == "a"):
        start(None, functools.partial(ag, f, p, 2, other_y))
    for p in PHASES[0]:
        start(z > 0, functools.partial(ag, f, p, 0, f - 2))
        start(z < n_z - 1, functools.partial(ag, f, p, 1, f + 2))
    for p in range(len(PIECES)):
        exchange(None, f, p)

    n_norm = n_tok // 64
    tok_copy.wait()

    @pl.loop(0, n_norm)
    def _(i):
        r = pl.multiple_of(i * 64, 64)
        x = tok[pl.ds(r, 64), :].astype(jnp.float32)
        x = x * lax.rsqrt(jnp.mean(x * x, axis=-1, keepdims=True) + eps_norm)
        x = x.astype(jnp.bfloat16)
        for j in range(n_z):
            normed[j, pl.ds(r, 64), :] = x[:, j * k_z : (j + 1) * k_z]

    def multiply(w, acc, zz, first):
        k0 = pl.multiple_of(zz * k_z, k_z)

        @pl.loop(0, n_tok // m_tile)
        def _(i):
            r = pl.multiple_of(i * m_tile, m_tile)
            a = normed[zz, pl.ds(r, m_tile), :]
            for c, n in col_tiles:
                v = jnp.dot(a, w[pl.ds(k0, k_z), c : c + n], preferred_element_type=jnp.float32)
                if first:
                    acc[pl.ds(r, m_tile), c : c + n] = v
                else:
                    acc[pl.ds(r, m_tile), c : c + n] += v

    def sides(d):
        return [(z >= d, z - d, -1), (z + d < n_z, z + d, 1)]

    def forward(cond, zz, sign, o, p):
        if sign < 0:
            start(jnp.logical_and(cond, z < n_z - 1), functools.partial(ag, o, p, 1, f + 2))
        else:
            start(jnp.logical_and(cond, z > 0), functools.partial(ag, o, p, 0, f - 2))

    def share_step(group, step):
        q, n, parts = GROUPS[group]
        share, half_in, out_send, out_in = shares[group], pairs[group], sends[group], ins[group]
        wide = n * part

        def aa_wait(c):
            for k in range(per):
                for p in parts:
                    _, h, m, _ = PIECES[p]
                    ref = down_o.at[
                        pl.ds(k * d_rows, d_rows), pl.ds(pl.multiple_of(c * d_cols + h * part, part), m * part)
                    ]
                    pltpu.make_async_remote_copy(
                        ref, ref, aa_send.at[0, p], aa_recv.at[c, k, p], device_id=(f, near), device_id_type=MESH,
                    ).wait_recv()

        def product(c, slot):
            @pl.loop(0, n_tok // m_tile)
            def _(i):
                r = pl.multiple_of(i * m_tile, m_tile)
                col = pl.multiple_of(c * d_cols + q * part, part)
                v = jnp.dot(hidden[pl.ds(r, m_tile), :], down_o[:, pl.ds(col, wide)], preferred_element_type=jnp.float32)
                share[slot, pl.ds(r, m_tile), :] = v.astype(jnp.bfloat16)

        def pair(slot):
            return pltpu.make_async_remote_copy(
                share.at[slot], half_in.at[slot], rs_send.at[group, slot], rs_recv.at[group, slot],
                device_id=(f, near), device_id_type=MESH,
            )

        def across():
            return pltpu.make_async_remote_copy(
                out_send, out_in, rs_send.at[group, 2], rs_recv.at[group, 2],
                device_id=(f, far), device_id_type=MESH,
            )

        if step == 0:
            aa_wait(far_near)
            product(far_near, 0)
            start(None, functools.partial(pair, 0))
        elif step == 1:
            aa_wait(far)
            product(far, 2)
            pair(0).wait_recv()
            out_send[...] = (share[2].astype(jnp.float32) + half_in[0].astype(jnp.float32)).astype(jnp.bfloat16)
            start(None, across)
        elif step == 2:
            aa_wait(near)
            product(near, 1)
            start(None, functools.partial(pair, 1))
        elif step == 3:
            product(t, 3)
        elif step == 4:
            pair(1).wait_recv()
            across().wait_recv()
            mix_o[:, q * part : (q + n) * part] = (
                share[3].astype(jnp.float32) + half_in[1].astype(jnp.float32) + out_in[...].astype(jnp.float32)
            ).astype(jnp.bfloat16)

    for _, _, what, d, p in plan(n_z):
        if what == "launch":
            launch(d)
        elif what == "share":
            share_step(d, p)
        elif what == "line":
            for cond, zz, sign in sides(d):
                o = zz * 2 + y
                pl.when(cond)(functools.partial(land, o, p))
                forward(cond, zz, sign, o, p)
                if kind(p) == "a":
                    start(cond, functools.partial(ag, o, p, 2, other_y))
                exchange(cond, o, p)
        elif what == "line_other":
            for cond, zz, sign in sides(d):
                o = zz * 2 + 1 - y
                pl.when(cond)(functools.partial(land, o, p))
                forward(cond, zz, sign, o, p)
                exchange(cond, o, p)
        elif what == "pair":
            if d == 0:
                land(other_y, p)
                exchange(None, other_y, p)
            else:
                for cond, zz, sign in sides(d):
                    o = zz * 2 + 1 - y
                    pl.when(cond)(functools.partial(land, o, p))
                    exchange(cond, o, p)
        elif what == "mul_gate" or what == "mul_up":
            w, acc = (gate_o, acc_g) if what == "mul_gate" else (up_o, acc_u)
            if d == 0:
                multiply(w, acc, z, True)
            else:
                for cond, zz, sign in sides(d):
                    pl.when(cond)(functools.partial(multiply, w, acc, zz, False))
        elif what == "act":
            @pl.loop(0, n_tok // 32)
            def _(i):
                r = pl.multiple_of(i * 32, 32)
                v = acc_g[pl.ds(r, 32), :]
                hidden[pl.ds(r, 32), :] = (v / (1.0 + jnp.exp(-v)) * acc_u[pl.ds(r, 32), :]).astype(jnp.bfloat16)

    for cond, make in started:
        if cond is None:
            make().wait_send()
        else:
            pl.when(cond)(lambda make=make: make().wait_send())


def on_device(n_fs, n_tp, tokens, norm_gain, gate_weight, up_weight, down_weight):
    n_tok, d_model = tokens.shape
    rows, width = gate_weight.shape
    d_rows, d_cols = down_weight.shape
    part = d_cols // 4
    n_z = n_fs // 2
    n_p = len(PIECES)
    bf = jnp.bfloat16
    vmem = pl.BlockSpec(memory_space=pltpu.VMEM)
    dma = pltpu.SemaphoreType.DMA
    return pl.pallas_call(
        functools.partial(kernel, n_fs, n_tp),
        out_shape=(
            pltpu.VMEM((d_model, width), bf),
            pltpu.VMEM((d_model, width), bf),
            pltpu.VMEM((d_rows * n_fs // n_tp, d_model), bf),
            pltpu.VMEM((n_tok, d_cols), bf),
        ),
        in_specs=[pl.BlockSpec(memory_space=pl.ANY)] + [vmem] * 4,
        out_specs=(vmem,) * 4,
        scratch_shapes=[
            pltpu.VMEM((n_tok, d_model), bf),
            pltpu.VMEM((n_fs, d_rows, d_cols), bf),
            pltpu.VMEM((n_z, n_tok, d_model // n_z), bf),
            pltpu.VMEM((n_tok, width), jnp.float32),
            pltpu.VMEM((n_tok, width), jnp.float32),
            pltpu.VMEM((n_tok, width), bf),
            *[pltpu.VMEM((4, n_tok, g[1] * part), bf) for g in GROUPS],
            *[pltpu.VMEM((2, n_tok, g[1] * part), bf) for g in GROUPS],
            *[pltpu.VMEM((n_tok, g[1] * part), bf) for g in GROUPS],
            *[pltpu.VMEM((n_tok, g[1] * part), bf) for g in GROUPS],
            dma,
            dma((n_fs, n_p, 3)),
            dma((n_fs, n_p)),
            dma((n_fs, n_p)),
            dma((n_tp, n_fs // n_tp, n_p)),
            dma((2, 3)),
            dma((2, 3)),
        ],
        compiler_params=pltpu.CompilerParams(
            collective_id=0, has_side_effects=True, vmem_limit_bytes=46 * 2**20
        ),
    )(tokens, norm_gain[None, :], gate_weight, up_weight, down_weight)


PARTS = (
    ("gate", 0, 8, "a"),
    ("gate", 8, 8, "a"),
    ("up", 0, 6, "a"),
    ("up", 6, 5, "a"),
    ("up", 11, 5, "b"),
    ("down", 0, 1, "a"),
    ("down", 1, 1, "a"),
    ("down", 2, 1, "a"),
    ("down", 3, 1, "b"),
)
DOWN = tuple(p for p in range(len(PARTS)) if PARTS[p][0] == "down")
FAR_GROUPS = ((0, 2), (2, 2))
NEAR_GROUPS = ((0, 2), (2, 1), (3, 1))
UNIT, LAG, LEAD = 7.73, 2.0, 16.0


def crossing(src, p, n_z):
    return PARTS[p][0] == "down" and 2 * src >= n_z


def reach(src, p, n_z):
    if crossing(src, p, n_z) or PARTS[p][3] == "a":
        return (src, src)
    return (0, n_z - 1)


def length(p):
    return UNIT * (0.5 if PARTS[p][0] == "down" else PARTS[p][2] / 8)


def rank(n_z, m, link, item):
    src, side, p = item
    if link == "x":
        return (0,)
    b = reach(src, p, n_z) != (src, src)
    if link == "y" and b:
        return (0, p)
    if PARTS[p][0] == "down":
        return (1 if crossing(src, p, n_z) else 4, p, abs(src - m), side)
    return (3 if b else 2, p, abs(src - m), side)


def simulate(n_z):
    queue, free, sent = {}, {}, {}
    events, have = [], [{} for _ in range(n_z)]
    far_in = [{} for _ in range(n_z)]
    count = [0]
    for m in range(n_z):
        for link in ("up", "dn", "y", "x"):
            queue[m, link], free[m, link], sent[m, link] = [], True, []

    def add(at, what, *rest):
        count[0] += 1
        heapq.heappush(events, (at, count[0], what, rest))

    def kick(at, m, link):
        if free[m, link] and queue[m, link]:
            queue[m, link].sort()
            _, item = queue[m, link].pop(0)
            free[m, link] = False
            sent[m, link].append((at, item))
            add(at + length(item[2]), "free", m, link)
            add(at + length(item[2]) + LAG, "land", m, link, item)

    def put(at, m, link, item):
        queue[m, link].append((rank(n_z, m, link, item), item))
        kick(at, m, link)

    def got(at, m, item):
        src, side, p = item
        have[m][item] = at
        low, high = reach(src, p, n_z)
        if m >= src and m < (n_z - 1 if side == 0 else high):
            put(at, m, "up", item)
        if m <= src and m > (0 if side == 0 else low):
            put(at, m, "dn", item)
        if side == 0 and (m == src or not low <= m <= high):
            put(at, m, "y", item)
        if crossing(src, p, n_z):
            put(at, m, "x", item)

    for m in range(n_z):
        for p in range(len(PARTS)):
            add(1.0 if PARTS[p][0] == "up" else 0.0, "own", m, (m, 0, p))
    while events:
        at, _, what, rest = heapq.heappop(events)
        if what == "own":
            got(at, *rest)
        elif what == "free":
            free[rest] = True
            kick(at, *rest)
        else:
            m, link, item = rest
            if link == "x":
                far_in[n_z - 1 - m][item] = at
            elif link == "y":
                got(at, m, (item[0], 1, item[2]))
            else:
                got(at, m + (1 if link == "up" else -1), item)
    return have, far_in, sent


def timetable(n_z):
    have, far_in, sent = simulate(n_z)
    sources, ready = {}, {}
    for m in range(n_z):
        for name in ("gate", "up"):
            mine = [p for p in range(len(PARTS)) if PARTS[p][0] == name]
            done = sorted((max(have[m][src, side, p] for side in (0, 1) for p in mine), src) for src in range(n_z))
            for j, (at, src) in enumerate(done):
                sources[m, name, j], ready[m, (name, j)] = src, at
        ready[m, ("lift", 0)] = 0.5
        ready[m, ("norm", 0)] = 1.5
        ready[m, ("act", 0)] = 0.0
        for g, (q, n) in enumerate(FAR_GROUPS):
            ready[m, ("far", g)] = max(at for item, at in far_in[m].items() if q <= PARTS[item[2]][1] < q + n)
        for g, (q, n) in enumerate(NEAR_GROUPS):
            ready[m, ("near", g)] = max(
                at for item, at in have[m].items()
                if PARTS[item[2]][0] == "down" and not crossing(item[0], item[2], n_z) and q <= PARTS[item[2]][1] < q + n
            )
        ready[m, ("end", 0)] = 1e9
    muls = sorted(
        (sum(ready[m, (name, j)] for m in range(n_z)), name, j) for name in ("gate", "up") for j in range(n_z)
    )
    steps = [("lift", 0), ("norm", 0)] + [(name, j) for _, name, j in muls] + [("act", 0)]
    steps += [("far", g) for g in range(len(FAR_GROUPS))] + [("near", g) for g in range(len(NEAR_GROUPS))] + [("end", 0)]
    spans = {"lift": 0.5, "norm": 3.0, "gate": 1.5, "up": 1.5, "act": 1.5, "far": 3.0, "near": 0.2, "end": 0.0}
    before = {}
    for m in range(n_z):
        todo = [(at, 0, "wait", item) for item, at in have[m].items() if item[:2] != (m, 0)]
        for link in ("up", "dn", "y", "x"):
            last = 0.0
            for at, item in sent[m, link]:
                last = max(last, have[m][item], at - LEAD)
                todo.append((last, 1, link, item))
        for item, at in have[m].items():
            if PARTS[item[2]][0] == "down" and not crossing(item[0], item[2], n_z):
                todo.append((at, 1, "core", item))
        todo.sort(key=lambda e: e[:2])
        now = 0.0
        for step in steps:
            now = max(now, ready[m, step])
            before[m, step] = [e[2:] for e in todo if e[0] <= now]
            todo = [e for e in todo if e[0] > now]
            now += spans[step[0]]
    return steps, sources, before


def line_kernel(
    n_fs, n_tp, tok_hbm, gain, gw_hbm, uw_hbm, dw_hbm, gate_o, up_o, down_o, dcol, hidden, hidden_near, out_in,
    tok, gw, uw, dw, normed, acc_g, acc_u, far_a, far_b, far_in, out_send,
    in_sem, ag_send, ag_recv, aa_send, aa_recv, fp_send, fp_recv, ac_send, ac_recv, hid_send, hid_recv,
):
    loads = [
        pltpu.make_async_copy(src, dst, in_sem.at[i])
        for i, (src, dst) in enumerate(((gw_hbm, gw), (dw_hbm, dw), (uw_hbm, uw), (tok_hbm, tok)))
    ]
    for load in loads:
        load.start()
    f, t = lax.axis_index("fs"), lax.axis_index("tp")
    n_z = n_fs // 2
    z, y = f // 2, f % 2
    x = t // 2
    per = n_fs // n_tp
    rows = gw.shape[0]
    d_rows, d_cols = dw.shape
    part = d_cols // 4
    n_tok = tok.shape[0]
    k_z = normed.shape[2]
    m_tile = min(256, n_tok)
    width = gw.shape[1]
    col_tiles = [(c, min(512, width - c)) for c in range(0, width, 512)]
    place = z + x * (n_z - 1 - 2 * z)
    ahead = f + 2 - 4 * x
    behind = f - 2 + 4 * x
    other_y = f + 1 - 2 * y
    near = t + 1 - 2 * (t % 2)
    far = t + 2 - 4 * x
    far_near = far + 1 - 2 * (far % 2)
    steps, sources, before = timetable(n_z)

    def z_of(src):
        return src + x * (n_z - 1 - 2 * src)

    def owner_of(item):
        src, side, _ = item
        return 2 * z_of(src) + (y if side == 0 else 1 - y)

    def view(o, p):
        name, first, n, _ = PARTS[p]
        if name == "down":
            return dcol.at[o, :, pl.ds(first * part, n * part)]
        ref = gate_o if name == "gate" else up_o
        step = rows // 16
        return ref.at[pl.ds(pl.multiple_of(o * rows + first * step, step), n * step), :]

    def ag(item, way, dest):
        o, p = owner_of(item), item[2]
        v = view(o, p)
        return pltpu.make_async_remote_copy(
            v, v, ag_send.at[o, p, way], ag_recv.at[o, p], device_id=(dest, t), device_id_type=MESH,
        )

    def hand(item):
        o, p = owner_of(item), item[2]
        _, first, n, _ = PARTS[p]
        row = pl.multiple_of((o % per) * d_rows, d_rows)
        col = pl.multiple_of(t * d_cols + first * part, part)
        return pltpu.make_async_remote_copy(
            view(o, p), down_o.at[pl.ds(row, d_rows), pl.ds(col, n * part)],
            aa_send.at[o, p], aa_recv.at[t, o % per, p],
            device_id=(f, o // per), device_id_type=MESH,
        )

    def transfer(what, item):
        if what == "up":
            return ag(item, 0, ahead)
        if what == "dn":
            return ag(item, 1, behind)
        if what == "y":
            return ag(item, 2, other_y)
        return hand(item)

    def elsewhere(item):
        return owner_of(item) // per != t

    def play(step):
        for m in range(n_z):
            def events(m=m):
                for what, item in before[m, step]:
                    if what == "wait":
                        ag(item, 0, f).wait_recv()
                    elif what == "core":
                        pl.when(elsewhere(item))(lambda item=item: hand(item).start())
                    else:
                        transfer(what, item).start()
            if before[m, step]:
                pl.when(place == m)(events)

    barrier = pltpu.get_barrier_semaphore()
    peers = [
        (z > 0, (f - 2, t)), (z < n_z - 1, (f + 2, t)), (None, (other_y, t)),
        (None, (f, near)), (None, (f, far)), (None, (f, far_near)),
    ]
    for cond, dev in peers:
        def hello(dev=dev):
            pl.semaphore_signal(barrier, inc=1, device_id=dev, device_id_type=MESH)
        hello() if cond is None else pl.when(cond)(hello)

    g = jnp.broadcast_to(gain[...], (8, rows)).T[:, :1]
    base = pl.multiple_of(f * rows, rows)
    loads[0].wait()
    gate_o[pl.ds(base, rows), :] = (gw[...] * g).astype(jnp.bfloat16)
    loads[1].wait()
    dcol[f] = dw[...].astype(jnp.bfloat16)
    inner = jnp.logical_and(z > 0, z < n_z - 1)
    pl.when(inner)(lambda: pl.semaphore_wait(barrier, len(peers)))
    pl.when(jnp.logical_not(inner))(lambda: pl.semaphore_wait(barrier, len(peers) - 1))

    def lift():
        loads[2].wait()
        up_o[pl.ds(base, rows), :] = (uw[...] * g).astype(jnp.bfloat16)

    def norm():
        loads[3].wait()

        @pl.loop(0, n_tok // 64)
        def _(i):
            r = pl.multiple_of(i * 64, 64)
            v = tok[pl.ds(r, 64), :].astype(jnp.float32)
            v = v * lax.rsqrt(jnp.mean(v * v, axis=-1, keepdims=True) + eps_norm)
            v = v.astype(jnp.bfloat16)
            for j in range(n_z):
                normed[j, pl.ds(r, 64), :] = v[:, j * k_z : (j + 1) * k_z]

    def multiply(w, acc, src, first):
        zz = z_of(src)
        k0 = pl.multiple_of(zz * k_z, k_z)

        @pl.loop(0, n_tok // m_tile)
        def _(i):
            r = pl.multiple_of(i * m_tile, m_tile)
            a = normed[zz, pl.ds(r, m_tile), :]
            for c, n in col_tiles:
                v = jnp.dot(a, w[pl.ds(k0, k_z), c : c + n], preferred_element_type=jnp.float32)
                if first:
                    acc[pl.ds(r, m_tile), c : c + n] = v
                else:
                    acc[pl.ds(r, m_tile), c : c + n] += v

    def act():
        @pl.loop(0, n_tok // 32)
        def _(i):
            r = pl.multiple_of(i * 32, 32)
            v = acc_g[pl.ds(r, 32), :]
            hidden[pl.ds(r, 32), :] = (v / (1.0 + jnp.exp(-v)) * acc_u[pl.ds(r, 32), :]).astype(jnp.bfloat16)

    def arrived(c, q, n):
        for k in range(per):
            for p in DOWN:
                _, first, m, _ = PARTS[p]
                if q <= first < q + n:
                    ref = down_o.at[
                        pl.ds(k * d_rows, d_rows), pl.ds(pl.multiple_of(c * d_cols + first * part, part), m * part)
                    ]
                    pltpu.make_async_remote_copy(
                        ref, ref, aa_send.at[0, p], aa_recv.at[c, k, p], device_id=(f, near), device_id_type=MESH,
                    ).wait_recv()

    def product(c, q, n, out):
        @pl.loop(0, n_tok // m_tile)
        def _(i):
            r = pl.multiple_of(i * m_tile, m_tile)
            col = pl.multiple_of(c * d_cols + q * part, part)
            v = jnp.dot(
                hidden[pl.ds(r, m_tile), :], down_o[:, pl.ds(col, n * part)], preferred_element_type=jnp.float32
            )
            out[pl.ds(r, m_tile), :] = v.astype(jnp.bfloat16)

    def cols(q, n):
        return slice(q * part, (q + n) * part)

    def far_pair(i):
        q, n = FAR_GROUPS[i]
        return pltpu.make_async_remote_copy(
            far_a.at[:, cols(q, n)], far_in.at[:, cols(q, n)], fp_send.at[i], fp_recv.at[i],
            device_id=(f, near), device_id_type=MESH,
        )

    def across(i):
        q, n = FAR_GROUPS[i]
        return pltpu.make_async_remote_copy(
            out_send.at[:, cols(q, n)], out_in.at[:, cols(q, n)], ac_send.at[i], ac_recv.at[i],
            device_id=(f, far), device_id_type=MESH,
        )

    def hidden_copy():
        return pltpu.make_async_remote_copy(
            hidden, hidden_near, hid_send, hid_recv, device_id=(f, near), device_id_type=MESH,
        )

    def far_step(i):
        q, n = FAR_GROUPS[i]
        arrived(far_near, q, n)
        product(far_near, q, n, far_a.at[:, cols(q, n)])
        far_pair(i).start()
        arrived(far, q, n)
        product(far, q, n, far_b.at[:, cols(q, n)])
        far_pair(i).wait_recv()
        out_send[:, cols(q, n)] = (
            far_b[:, cols(q, n)].astype(jnp.float32) + far_in[:, cols(q, n)].astype(jnp.float32)
        ).astype(jnp.bfloat16)
        across(i).start()

    def near_step(i):
        q, n = NEAR_GROUPS[i]
        col = pl.multiple_of(t * d_cols + q * part, part)
        for k in range(per):
            down_o[k * d_rows : (k + 1) * d_rows, pl.ds(col, n * part)] = dcol[t * per + k, :, cols(q, n)]

    def end():
        arrived(near, 0, 4)
        for i in range(len(FAR_GROUPS)):
            across(i).wait_recv()
        hidden_copy().wait_recv()

    done = {"gate": 0, "up": 0}
    for step in steps:
        play(step)
        what, i = step
        if what == "lift":
            lift()
        elif what == "norm":
            norm()
        elif what == "act":
            act()
            hidden_copy().start()
        elif what == "far":
            far_step(i)
        elif what == "near":
            near_step(i)
        elif what == "end":
            end()
        else:
            src = sources[0, what, i]
            for m in range(1, n_z):
                src = jnp.where(place == m, sources[m, what, i], src)
            multiply(gate_o if what == "gate" else up_o, acc_g if what == "gate" else acc_u, src, done[what] == 0)
            done[what] += 1

    for i in range(len(FAR_GROUPS)):
        far_pair(i).wait_send()
        across(i).wait_send()
    hidden_copy().wait_send()
    for m in range(n_z):
        @pl.when(place == m)
        def _(m=m):
            for step in steps:
                for what, item in before[m, step]:
                    if what == "core":
                        pl.when(elsewhere(item))(lambda item=item: hand(item).wait_send())
                    elif what != "wait":
                        transfer(what, item).wait_send()


def finish(
    n_tp, gate_i, up_i, down_i, dcol, hidden, hidden_near, out_in, gate_o, up_o, down_o, mix_o, near_w, mix, sems,
):
    t = lax.axis_index("tp")
    near = t + 1 - 2 * (t % 2)
    per = dcol.shape[0] // n_tp
    d_rows, d_cols = dcol.shape[1:]
    n_tok = hidden.shape[0]
    m_tile = min(256, n_tok)
    copies = [
        pltpu.make_async_copy(src, dst, sems.at[i])
        for i, (src, dst) in enumerate(((gate_i, gate_o), (up_i, up_o), (down_i, down_o), (mix, mix_o)))
    ]
    for copy in copies[:3]:
        copy.start()
    for k in range(per):
        near_w[k * d_rows : (k + 1) * d_rows, :] = dcol[near * per + k]
    col = pl.multiple_of(t * d_cols, d_cols)

    @pl.loop(0, n_tok // m_tile)
    def _(i):
        r = pl.ds(pl.multiple_of(i * m_tile, m_tile), m_tile)
        own = jnp.dot(hidden[r, :], down_i[:, pl.ds(col, d_cols)], preferred_element_type=jnp.float32)
        other = jnp.dot(hidden_near[r, :], near_w[...], preferred_element_type=jnp.float32)
        own, other = own.astype(jnp.bfloat16).astype(jnp.float32), other.astype(jnp.bfloat16).astype(jnp.float32)
        mix[r, :] = (own + other + out_in[r, :].astype(jnp.float32)).astype(jnp.bfloat16)

    copies[3].start()
    for copy in copies:
        copy.wait()


def line_on_device(n_fs, n_tp, tokens, norm_gain, gate_weight, up_weight, down_weight):
    n_tok, d_model = tokens.shape
    rows, width = gate_weight.shape
    d_rows, d_cols = down_weight.shape
    n_z = n_fs // 2
    n_p = len(PARTS)
    bf = jnp.bfloat16
    vmem = pl.BlockSpec(memory_space=pltpu.VMEM)
    dma = pltpu.SemaphoreType.DMA
    n_far = len(FAR_GROUPS)
    hbm = pl.BlockSpec(memory_space=pl.ANY)
    d_own = d_rows * n_fs // n_tp
    shapes = (
        (d_model, width), (d_model, width), (d_own, d_model), (n_fs, d_rows, d_cols),
        (n_tok, width), (n_tok, width), (n_tok, d_cols),
    )
    held = pl.pallas_call(
        functools.partial(line_kernel, n_fs, n_tp),
        out_shape=tuple(pltpu.VMEM(shape, bf) for shape in shapes),
        in_specs=[hbm, vmem, hbm, hbm, hbm],
        out_specs=(vmem,) * len(shapes),
        scratch_shapes=[
            pltpu.VMEM((n_tok, d_model), bf),
            pltpu.VMEM((rows, width), jnp.float32),
            pltpu.VMEM((rows, width), jnp.float32),
            pltpu.VMEM((d_rows, d_cols), jnp.float32),
            pltpu.VMEM((n_z, n_tok, d_model // n_z), bf),
            pltpu.VMEM((n_tok, width), jnp.float32),
            pltpu.VMEM((n_tok, width), jnp.float32),
            *[pltpu.VMEM((n_tok, d_cols), bf)] * 4,
            dma((4,)),
            dma((n_fs, n_p, 3)),
            dma((n_fs, n_p)),
            dma((n_fs, n_p)),
            dma((n_tp, n_fs // n_tp, n_p)),
            dma((n_far,)),
            dma((n_far,)),
            dma((n_far,)),
            dma((n_far,)),
            dma,
            dma,
        ],
        compiler_params=pltpu.CompilerParams(
            collective_id=0, has_side_effects=True, vmem_limit_bytes=30 * 2**20
        ),
    )(tokens, norm_gain[None, :], gate_weight, up_weight, down_weight)
    return pl.pallas_call(
        functools.partial(finish, n_tp),
        out_shape=tuple(
            jax.ShapeDtypeStruct(shape, bf)
            for shape in ((d_model, width), (d_model, width), (d_own, d_model), (n_tok, d_cols))
        ),
        in_specs=[vmem] * len(shapes),
        out_specs=(hbm,) * 4,
        scratch_shapes=[pltpu.VMEM((d_own, d_cols), bf), pltpu.VMEM((n_tok, d_cols), bf), dma((4,))],
        compiler_params=pltpu.CompilerParams(vmem_limit_bytes=6 * 2**20),
    )(*held)


def solution(mesh):
    n_fs, n_tp = mesh.shape["fs"], mesh.shape["tp"]
    in_specs = (P("fs", None), P("fs"), P("fs", "tp"), P("fs", "tp"), P("fs", "tp"))
    out_specs = (P(None, "tp"), P(None, "tp"), P("tp", None), P("fs", "tp"))
    body = line_on_device if (n_fs, n_tp) == (8, 4) else on_device
    return jax.shard_map(
        functools.partial(body, n_fs, n_tp), mesh=mesh, in_specs=in_specs, out_specs=out_specs, check_vma=False
    )
```

```python
import functools
import heapq

import jax
import jax.numpy as jnp
from jax import lax
from jax.experimental import pallas as pl
from jax.experimental.pallas import tpu as pltpu
from jax.sharding import PartitionSpec as P

eps_norm = 1e-06
MESH = pl.DeviceIdType.MESH

PIECES = (
    ("gate", 0, 1, "a"),
    ("gate", 1, 1, "a"),
    ("down", 2, 2, "b"),
    ("up", 0, 1, "a"),
    ("up", 1, 1, "a"),
    ("down", 0, 1, "a"),
    ("down", 1, 1, "a"),
)
PHASES = ((0, 1, 6), (2,), (3, 4), (5,))
GROUPS = ((1, 3, (2, 6)), (0, 1, (5,)))


def cost(p):
    return 0.5 if PIECES[p][0] == "down" and kind(p) == 1 else 1.0


def kind(p):
    return PIECES[p][3]


def plan(n_z):
    events = []
    seq = [(d, p) for phase in PHASES for d in range(1, n_z) for p in phase]
    order = sorted(range(len(PIECES)), key=lambda p: kind(p) == "a")
    own, total = {}, 0.0
    for p in order:
        total += cost(p)
        own[p] = total
    z_time, now = {}, 0.0
    for i, phase in enumerate(PHASES):
        for d in range(1, n_z):
            if d == n_z - 1 and i + 1 < len(PHASES):
                events.append((now + 0.02, 1, "launch", i + 1, 0))
            for p in phase:
                if kind(p) == "a":
                    now += cost(p)
                    z_time[d, p] = now
                    events.append((now, 0, "line", d, p))
                else:
                    now += 2.0 * cost(p)
                    z_time[d, p] = now
                    events.append((now - cost(p), 0, "line", d, p))
                    events.append((now, 0, "line_other", d, p))
    y_time = {}
    for z in range(n_z):
        at = total
        for d, p in seq:
            if kind(p) == "a":
                for zz in (z - d, z + d):
                    if 0 <= zz < n_z:
                        at = max(at, z_time[d, p]) + cost(p)
                        y_time[d, p] = max(y_time.get((d, p), 0.0), at)
    for p, at in own.items():
        events.append((at, 1, "pair", 0, p))
    for (d, p), at in y_time.items():
        events.append((at, 1, "pair", d, p))
    here = dict(y_time)
    here.update({(0, p): at for p, at in own.items()})
    last = 0.0
    for name in ("gate", "up"):
        mine = [p for p in range(len(PIECES)) if PIECES[p][0] == name]
        for d in range(n_z):
            at = max(here[d, p] for p in mine) + 0.01
            events.append((at, 2, "mul_" + name, d, 0))
            last = max(last, at)
    events.append((last + 0.01, 3, "act", 0, 0))
    end = max(e[0] for e in events) + 0.1
    for step in range(4):
        events.append((end + 0.01 + 0.01 * step, 4, "share", 0, step))
    for step in range(5):
        events.append((end + 0.1 + 0.1 * step, 4, "share", 1, step))
    events.append((end + 0.35, 4, "share", 0, 4))
    return sorted(events)


def kernel(
    n_fs, n_tp, tok_hbm, gain, gw, uw, dw, gate_o, up_o, down_o, mix_o,
    tok, dcol, normed, acc_g, acc_u, hidden, share0, share1, pair0, pair1, send0, send1, in0, in1,
    tok_sem, ag_send, ag_recv, aa_send, aa_recv, rs_send, rs_recv,
):
    tok_copy = pltpu.make_async_copy(tok_hbm, tok, tok_sem)
    tok_copy.start()
    shares, pairs, sends, ins = (share0, share1), (pair0, pair1), (send0, send1), (in0, in1)
    f, t = lax.axis_index("fs"), lax.axis_index("tp")
    n_z = n_fs // 2
    z, y = f // 2, f % 2
    per = n_fs // n_tp
    rows = gw.shape[0]
    d_rows, d_cols = dw.shape
    part = d_cols // 4
    n_tok = tok.shape[0]
    k_z = normed.shape[2]
    m_tile = min(256, n_tok)
    width = gw.shape[1]
    col_tiles = [(c, min(512, width - c)) for c in range(0, width, 512)]

    def flip(bit):
        return t + bit - 2 * bit * ((t // bit) % 2)

    near, far = flip(1), flip(2)
    far_near = far + 1 - 2 * (far % 2)

    def view(o, p):
        name, h, n, _ = PIECES[p]
        if name == "down":
            return dcol.at[o, :, pl.ds(h * part, n * part)]
        ref = gate_o if name == "gate" else up_o
        return ref.at[pl.ds(pl.multiple_of(o * rows + h * (rows // 2), rows // 2), rows // 2), :]

    def ag(o, p, way, dest):
        v = view(o, p)
        return pltpu.make_async_remote_copy(
            v, v, ag_send.at[o, p, way], ag_recv.at[o, p],
            device_id=(dest, t), device_id_type=MESH,
        )

    started = []

    def start(cond, make):
        if cond is None:
            make().start()
        else:
            pl.when(cond)(lambda: make().start())
        started.append((cond, make))

    def land(o, p):
        ag(o, p, 0, f).wait_recv()

    def exchange(cond, o, p):
        name, h, n, _ = PIECES[p]
        if name != "down":
            return
        owner = o // per
        k = o % per
        row = pl.multiple_of(k * d_rows, d_rows)
        col = pl.multiple_of(t * d_cols + h * part, part)

        def make():
            return pltpu.make_async_remote_copy(
                view(o, p), down_o.at[pl.ds(row, d_rows), pl.ds(col, n * part)],
                aa_send.at[o, p], aa_recv.at[t, k, p],
                device_id=(f, owner), device_id_type=MESH,
            )

        away = owner != t
        start(away if cond is None else jnp.logical_and(cond, away), make)
        mine = owner == t

        @pl.when(mine if cond is None else jnp.logical_and(cond, mine))
        def _():
            down_o[pl.ds(row, d_rows), pl.ds(col, n * part)] = dcol[o, :, h * part : (h + n) * part]

    barrier = pltpu.get_barrier_semaphore()
    other_y = f + 1 - 2 * y
    peers = [
        (z > 0, (f - 2, t)), (z < n_z - 1, (f + 2, t)), (None, (other_y, t)),
        (None, (f, near)), (None, (f, far)), (None, (f, far_near)),
    ]
    for cond, dev in peers:
        def hello(dev=dev):
            pl.semaphore_signal(barrier, inc=1, device_id=dev, device_id_type=MESH)
        hello() if cond is None else pl.when(cond)(hello)

    g = jnp.broadcast_to(gain[...], (8, rows)).T[:, :1]
    base = pl.multiple_of(f * rows, rows)
    gate_o[pl.ds(base, rows), :] = (gw[...] * g).astype(jnp.bfloat16)
    dcol[f] = dw[...].astype(jnp.bfloat16)
    up_o[pl.ds(base, rows), :] = (uw[...] * g).astype(jnp.bfloat16)
    inner = jnp.logical_and(z > 0, z < n_z - 1)
    pl.when(inner)(lambda: pl.semaphore_wait(barrier, len(peers)))
    pl.when(jnp.logical_not(inner))(lambda: pl.semaphore_wait(barrier, len(peers) - 1))

    def launch(phase):
        for p in PHASES[phase]:
            start(z > 0, functools.partial(ag, f, p, 0, f - 2))
            start(z < n_z - 1, functools.partial(ag, f, p, 1, f + 2))
            if kind(p) == "b":
                other_b(p)

    def other_b(p):
        start(z > 0, functools.partial(ag, other_y, p, 0, f - 2))
        start(z < n_z - 1, functools.partial(ag, other_y, p, 1, f + 2))

    for p in sorted(range(len(PIECES)), key=lambda p: kind(p) == "a"):
        start(None, functools.partial(ag, f, p, 2, other_y))
    for p in PHASES[0]:
        start(z > 0, functools.partial(ag, f, p, 0, f - 2))
        start(z < n_z - 1, functools.partial(ag, f, p, 1, f + 2))
    for p in range(len(PIECES)):
        exchange(None, f, p)

    n_norm = n_tok // 64
    tok_copy.wait()

    @pl.loop(0, n_norm)
    def _(i):
        r = pl.multiple_of(i * 64, 64)
        x = tok[pl.ds(r, 64), :].astype(jnp.float32)
        x = x * lax.rsqrt(jnp.mean(x * x, axis=-1, keepdims=True) + eps_norm)
        x = x.astype(jnp.bfloat16)
        for j in range(n_z):
            normed[j, pl.ds(r, 64), :] = x[:, j * k_z : (j + 1) * k_z]

    def multiply(w, acc, zz, first):
        k0 = pl.multiple_of(zz * k_z, k_z)

        @pl.loop(0, n_tok // m_tile)
        def _(i):
            r = pl.multiple_of(i * m_tile, m_tile)
            a = normed[zz, pl.ds(r, m_tile), :]
            for c, n in col_tiles:
                v = jnp.dot(a, w[pl.ds(k0, k_z), c : c + n], preferred_element_type=jnp.float32)
                if first:
                    acc[pl.ds(r, m_tile), c : c + n] = v
                else:
                    acc[pl.ds(r, m_tile), c : c + n] += v

    def sides(d):
        return [(z >= d, z - d, -1), (z + d < n_z, z + d, 1)]

    def forward(cond, zz, sign, o, p):
        if sign < 0:
            start(jnp.logical_and(cond, z < n_z - 1), functools.partial(ag, o, p, 1, f + 2))
        else:
            start(jnp.logical_and(cond, z > 0), functools.partial(ag, o, p, 0, f - 2))

    def share_step(group, step):
        q, n, parts = GROUPS[group]
        share, half_in, out_send, out_in = shares[group], pairs[group], sends[group], ins[group]
        wide = n * part

        def aa_wait(c):
            for k in range(per):
                for p in parts:
                    _, h, m, _ = PIECES[p]
                    ref = down_o.at[
                        pl.ds(k * d_rows, d_rows), pl.ds(pl.multiple_of(c * d_cols + h * part, part), m * part)
                    ]
                    pltpu.make_async_remote_copy(
                        ref, ref, aa_send.at[0, p], aa_recv.at[c, k, p], device_id=(f, near), device_id_type=MESH,
                    ).wait_recv()

        def product(c, slot):
            @pl.loop(0, n_tok // m_tile)
            def _(i):
                r = pl.multiple_of(i * m_tile, m_tile)
                col = pl.multiple_of(c * d_cols + q * part, part)
                v = jnp.dot(hidden[pl.ds(r, m_tile), :], down_o[:, pl.ds(col, wide)], preferred_element_type=jnp.float32)
                share[slot, pl.ds(r, m_tile), :] = v.astype(jnp.bfloat16)

        def pair(slot):
            return pltpu.make_async_remote_copy(
                share.at[slot], half_in.at[slot], rs_send.at[group, slot], rs_recv.at[group, slot],
                device_id=(f, near), device_id_type=MESH,
            )

        def across():
            return pltpu.make_async_remote_copy(
                out_send, out_in, rs_send.at[group, 2], rs_recv.at[group, 2],
                device_id=(f, far), device_id_type=MESH,
            )

        if step == 0:
            aa_wait(far_near)
            product(far_near, 0)
            start(None, functools.partial(pair, 0))
        elif step == 1:
            aa_wait(far)
            product(far, 2)
            pair(0).wait_recv()
            out_send[...] = (share[2].astype(jnp.float32) + half_in[0].astype(jnp.float32)).astype(jnp.bfloat16)
            start(None, across)
        elif step == 2:
            aa_wait(near)
            product(near, 1)
            start(None, functools.partial(pair, 1))
        elif step == 3:
            product(t, 3)
        elif step == 4:
            pair(1).wait_recv()
            across().wait_recv()
            mix_o[:, q * part : (q + n) * part] = (
                share[3].astype(jnp.float32) + half_in[1].astype(jnp.float32) + out_in[...].astype(jnp.float32)
            ).astype(jnp.bfloat16)

    for _, _, what, d, p in plan(n_z):
        if what == "launch":
            launch(d)
        elif what == "share":
            share_step(d, p)
        elif what == "line":
            for cond, zz, sign in sides(d):
                o = zz * 2 + y
                pl.when(cond)(functools.partial(land, o, p))
                forward(cond, zz, sign, o, p)
                if kind(p) == "a":
                    start(cond, functools.partial(ag, o, p, 2, other_y))
                exchange(cond, o, p)
        elif what == "line_other":
            for cond, zz, sign in sides(d):
                o = zz * 2 + 1 - y
                pl.when(cond)(functools.partial(land, o, p))
                forward(cond, zz, sign, o, p)
                exchange(cond, o, p)
        elif what == "pair":
            if d == 0:
                land(other_y, p)
                exchange(None, other_y, p)
            else:
                for cond, zz, sign in sides(d):
                    o = zz * 2 + 1 - y
                    pl.when(cond)(functools.partial(land, o, p))
                    exchange(cond, o, p)
        elif what == "mul_gate" or what == "mul_up":
            w, acc = (gate_o, acc_g) if what == "mul_gate" else (up_o, acc_u)
            if d == 0:
                multiply(w, acc, z, True)
            else:
                for cond, zz, sign in sides(d):
                    pl.when(cond)(functools.partial(multiply, w, acc, zz, False))
        elif what == "act":
            @pl.loop(0, n_tok // 32)
            def _(i):
                r = pl.multiple_of(i * 32, 32)
                v = acc_g[pl.ds(r, 32), :]
                hidden[pl.ds(r, 32), :] = (v / (1.0 + jnp.exp(-v)) * acc_u[pl.ds(r, 32), :]).astype(jnp.bfloat16)

    for cond, make in started:
        if cond is None:
            make().wait_send()
        else:
            pl.when(cond)(lambda make=make: make().wait_send())


def on_device(n_fs, n_tp, tokens, norm_gain, gate_weight, up_weight, down_weight):
    n_tok, d_model = tokens.shape
    rows, width = gate_weight.shape
    d_rows, d_cols = down_weight.shape
    part = d_cols // 4
    n_z = n_fs // 2
    n_p = len(PIECES)
    bf = jnp.bfloat16
    vmem = pl.BlockSpec(memory_space=pltpu.VMEM)
    dma = pltpu.SemaphoreType.DMA
    return pl.pallas_call(
        functools.partial(kernel, n_fs, n_tp),
        out_shape=(
            pltpu.VMEM((d_model, width), bf),
            pltpu.VMEM((d_model, width), bf),
            pltpu.VMEM((d_rows * n_fs // n_tp, d_model), bf),
            pltpu.VMEM((n_tok, d_cols), bf),
        ),
        in_specs=[pl.BlockSpec(memory_space=pl.ANY)] + [vmem] * 4,
        out_specs=(vmem,) * 4,
        scratch_shapes=[
            pltpu.VMEM((n_tok, d_model), bf),
            pltpu.VMEM((n_fs, d_rows, d_cols), bf),
            pltpu.VMEM((n_z, n_tok, d_model // n_z), bf),
            pltpu.VMEM((n_tok, width), jnp.float32),
            pltpu.VMEM((n_tok, width), jnp.float32),
            pltpu.VMEM((n_tok, width), bf),
            *[pltpu.VMEM((4, n_tok, g[1] * part), bf) for g in GROUPS],
            *[pltpu.VMEM((2, n_tok, g[1] * part), bf) for g in GROUPS],
            *[pltpu.VMEM((n_tok, g[1] * part), bf) for g in GROUPS],
            *[pltpu.VMEM((n_tok, g[1] * part), bf) for g in GROUPS],
            dma,
            dma((n_fs, n_p, 3)),
            dma((n_fs, n_p)),
            dma((n_fs, n_p)),
            dma((n_tp, n_fs // n_tp, n_p)),
            dma((2, 3)),
            dma((2, 3)),
        ],
        compiler_params=pltpu.CompilerParams(
            collective_id=0, has_side_effects=True, vmem_limit_bytes=46 * 2**20
        ),
    )(tokens, norm_gain[None, :], gate_weight, up_weight, down_weight)


PARTS = (
    ("gate", 0, 8),
    ("gate", 8, 8),
    ("up", 0, 8),
    ("up", 8, 4),
    ("up", 12, 4),
    ("down", 0, 1),
    ("down", 1, 1),
    ("down", 2, 1),
    ("down", 3, 1),
)
REACH = (
    ((0, 2), (0, 2), (0, 1), (0, 3), (0, 1), (0, 0), (0, 0), (0, 0), (0, 0)),
    ((1, 1), (1, 3), (1, 1), (1, 1), (1, 1), (1, 1), (0, 3), (0, 1), (1, 1)),
    ((2, 2), (2, 2), (2, 2), (2, 2), (2, 2), (2, 3), (0, 3), (2, 2), (2, 2)),
    ((2, 3), (2, 3), (0, 3), (3, 3), (2, 3), (3, 3), (0, 3), (3, 3), (1, 3)),
)
RANKS = (
    (0.98, 2.75, 3.09, 4.72, 2.28, 7.34, 5.35, 5.05, 5.57),
    (-0.59, 0.97, 3.70, 3.76, 0.58, 8.74, 11.15, 6.05, 10.14),
    (2.58, 3.18, 1.14, 4.50, 1.86, 1.38, 1.00, 0.63, 2.20),
    (4.44, 4.79, 5.54, 4.72, 3.65, 0.90, 4.97, 3.57, 3.69),
)
CROSS = (
    (1.79, 1.76, 1.17, 0.05, -0.15, 1.84, 1.49, 3.23, 0.29),
    (1.91, 0.67, 1.91, 2.54, 2.95, 0.66, 1.52, 0.56, 2.95),
    (-0.24, 2.08, 0.64, 2.98, 3.67, -0.32, 1.30, -0.30, 0.21),
    (0.46, 0.19, 3.29, 3.55, 2.08, 2.08, 1.84, 1.78, -0.37),
)
OTHER_SIDE = -0.3
DOWN = tuple(p for p in range(len(PARTS)) if PARTS[p][0] == "down")
FAR_GROUPS = ((0, 2), (2, 2))
NEAR_GROUPS = ((0, 2), (2, 1), (3, 1))
UNIT, LAG, LEAD = 7.73, 2.0, 16.0
WAYS = ("up", "dn", "y", "x")
RING = 6


def crossing(src, p, n_z):
    return PARTS[p][0] == "down" and 2 * src >= n_z


def length(p):
    return UNIT * (0.5 if PARTS[p][0] == "down" else PARTS[p][2] / 8)


def rank(m, link, item):
    src, side, p = item
    if link == "y" and REACH[src][p] != (src, src):
        return CROSS[src][p]
    return RANKS[src][p] + OTHER_SIDE * side + 0.01 * abs(src - m)


def simulate(n_z):
    queue, free, sent = {}, {}, {}
    events, have = [], [{} for _ in range(n_z)]
    far_in = [{} for _ in range(n_z)]
    count = [0]
    for m in range(n_z):
        for link in ("up", "dn", "y", "x"):
            queue[m, link], free[m, link], sent[m, link] = [], True, []

    def add(at, what, *rest):
        count[0] += 1
        heapq.heappush(events, (at, count[0], what, rest))

    def kick(at, m, link):
        if free[m, link] and queue[m, link]:
            queue[m, link].sort()
            _, item = queue[m, link].pop(0)
            free[m, link] = False
            sent[m, link].append((at, item))
            add(at + length(item[2]), "free", m, link)
            add(at + length(item[2]) + LAG, "land", m, link, item)

    def put(at, m, link, item):
        queue[m, link].append((rank(m, link, item), item))
        kick(at, m, link)

    def got(at, m, item):
        src, side, p = item
        have[m][item] = at
        low, high = REACH[src][p]
        if m >= src and m < (n_z - 1 if side == 0 else high):
            put(at, m, "up", item)
        if m <= src and m > (0 if side == 0 else low):
            put(at, m, "dn", item)
        if side == 0 and (m == src or not low <= m <= high):
            put(at, m, "y", item)
        if crossing(src, p, n_z):
            put(at, m, "x", item)

    for m in range(n_z):
        for p in range(len(PARTS)):
            add(1.0 if PARTS[p][0] == "up" else 0.0, "own", m, (m, 0, p))
    while events:
        at, _, what, rest = heapq.heappop(events)
        if what == "own":
            got(at, *rest)
        elif what == "free":
            free[rest] = True
            kick(at, *rest)
        else:
            m, link, item = rest
            if link == "x":
                far_in[n_z - 1 - m][item] = at
            elif link == "y":
                got(at, m, (item[0], 1, item[2]))
            else:
                got(at, m + (1 if link == "up" else -1), item)
    return have, far_in, sent


def timetable(n_z):
    have, far_in, sent = simulate(n_z)
    sources, ready = {}, {}
    for m in range(n_z):
        for name in ("gate", "up"):
            mine = [p for p in range(len(PARTS)) if PARTS[p][0] == name]
            done = sorted((max(have[m][src, side, p] for side in (0, 1) for p in mine), src) for src in range(n_z))
            for j, (at, src) in enumerate(done):
                sources[m, name, j], ready[m, (name, j)] = src, at
        ready[m, ("lift", 0)] = 0.5
        ready[m, ("norm", 0)] = 1.5
        ready[m, ("act", 0)] = 0.0
        for g, (q, n) in enumerate(FAR_GROUPS):
            ready[m, ("far", g)] = max(at for item, at in far_in[m].items() if q <= PARTS[item[2]][1] < q + n)
        for g, (q, n) in enumerate(NEAR_GROUPS):
            ready[m, ("near", g)] = max(
                at for item, at in have[m].items()
                if PARTS[item[2]][0] == "down" and not crossing(item[0], item[2], n_z) and q <= PARTS[item[2]][1] < q + n
            )
        ready[m, ("end", 0)] = 1e9
    muls = sorted(
        (sum(ready[m, (name, j)] for m in range(n_z)), name, j) for name in ("gate", "up") for j in range(n_z)
    )
    steps = [("lift", 0), ("norm", 0)] + [(name, j) for _, name, j in muls] + [("act", 0)]
    steps += [("far", g) for g in range(len(FAR_GROUPS))] + [("near", g) for g in range(len(NEAR_GROUPS))] + [("end", 0)]
    spans = {"lift": 0.5, "norm": 3.0, "gate": 1.5, "up": 1.5, "act": 1.5, "far": 3.0, "near": 0.2, "end": 0.0}
    before = {}
    for m in range(n_z):
        todo = [(at, 0, "wait", item) for item, at in have[m].items() if item[:2] != (m, 0)]
        for link in WAYS:
            last = 0.0
            for i, (at, item) in enumerate(sent[m, link]):
                last = max(last, have[m][item], at - LEAD)
                todo.append((last, 1, link, i))
        for item, at in have[m].items():
            if PARTS[item[2]][0] == "down" and not crossing(item[0], item[2], n_z):
                todo.append((at, 1, "core", item))
        todo.sort(key=lambda e: e[:2])
        now = 0.0
        for step in steps:
            now = max(now, ready[m, step])
            before[m, step] = [e[2:] for e in todo if e[0] <= now]
            todo = [e for e in todo if e[0] > now]
            now += spans[step[0]]
    items = {key: [item for _, item in log] for key, log in sent.items()}
    return steps, sources, before, items


def line_kernel(
    n_fs, n_tp, tok_hbm, gain, gw_hbm, uw_hbm, dw_hbm, gate_o, up_o, down_o, dcol, hidden, hidden_near, out_in,
    tok, gw, uw, dw, normed, acc_g, acc_u, far_a, far_b, far_in, out_send,
    in_sem, link_send, core_send, ag_recv, aa_recv, fp_send, fp_recv, ac_send, ac_recv, hid_send, hid_recv,
):
    loads = [
        pltpu.make_async_copy(src, dst, in_sem.at[i])
        for i, (src, dst) in enumerate(((gw_hbm, gw), (dw_hbm, dw), (uw_hbm, uw), (tok_hbm, tok)))
    ]
    for load in loads:
        load.start()
    f, t = lax.axis_index("fs"), lax.axis_index("tp")
    n_z = n_fs // 2
    z, y = f // 2, f % 2
    x = t // 2
    per = n_fs // n_tp
    rows = gw.shape[0]
    d_rows, d_cols = dw.shape
    part = d_cols // 4
    n_tok = tok.shape[0]
    k_z = normed.shape[2]
    m_tile = min(256, n_tok)
    width = gw.shape[1]
    col_tiles = [(c, min(512, width - c)) for c in range(0, width, 512)]
    place = z + x * (n_z - 1 - 2 * z)
    ahead = f + 2 - 4 * x
    behind = f - 2 + 4 * x
    other_y = f + 1 - 2 * y
    near = t + 1 - 2 * (t % 2)
    far = t + 2 - 4 * x
    far_near = far + 1 - 2 * (far % 2)
    steps, sources, before, items = timetable(n_z)

    def z_of(src):
        return src + x * (n_z - 1 - 2 * src)

    def owner_of(item):
        src, side, _ = item
        return 2 * z_of(src) + (y if side == 0 else 1 - y)

    def view(o, p):
        name, first, n = PARTS[p]
        if name == "down":
            return dcol.at[o, :, pl.ds(first * part, n * part)]
        ref = gate_o if name == "gate" else up_o
        step = rows // 16
        return ref.at[pl.ds(pl.multiple_of(o * rows + first * step, step), n * step), :]

    def ag(item, send, dest):
        o, p = owner_of(item), item[2]
        v = view(o, p)
        return pltpu.make_async_remote_copy(
            v, v, send, ag_recv.at[o, p], device_id=(dest, t), device_id_type=MESH,
        )

    def hand(item, send):
        o, p = owner_of(item), item[2]
        _, first, n = PARTS[p]
        group = [q <= first < q + m for q, m in FAR_GROUPS].index(True)
        lane = (t + o // per) % 2 * len(FAR_GROUPS) + group if crossing(item[0], p, n_z) else 2 * len(FAR_GROUPS)
        row = pl.multiple_of((o % per) * d_rows, d_rows)
        col = pl.multiple_of(t * d_cols + first * part, part)
        return pltpu.make_async_remote_copy(
            view(o, p), down_o.at[pl.ds(row, d_rows), pl.ds(col, n * part)],
            send, aa_recv.at[lane], device_id=(f, o // per), device_id_type=MESH,
        )

    def transfer(m, what, i):
        item, send = items[m, what][i], link_send.at[WAYS.index(what), i % RING]
        if what == "x":
            return hand(item, send)
        return ag(item, send, {"up": ahead, "dn": behind, "y": other_y}[what])

    def to_core(item):
        return hand(item, core_send.at[item[1] * len(DOWN) + DOWN.index(item[2])])

    def elsewhere(item):
        return owner_of(item) // per != t

    def play(step):
        for m in range(n_z):
            def events(m=m):
                for what, item in before[m, step]:
                    if what == "wait":
                        ag(item, link_send.at[0, 0], f).wait_recv()
                    elif what == "core":
                        pl.when(elsewhere(item))(lambda item=item: to_core(item).start())
                    else:
                        if item >= RING:
                            transfer(m, what, item - RING).wait_send()
                        transfer(m, what, item).start()
            if before[m, step]:
                pl.when(place == m)(events)

    barrier = pltpu.get_barrier_semaphore()
    peers = [
        (z > 0, (f - 2, t)), (z < n_z - 1, (f + 2, t)), (None, (other_y, t)),
        (None, (f, near)), (None, (f, far)), (None, (f, far_near)),
    ]
    for cond, dev in peers:
        def hello(dev=dev):
            pl.semaphore_signal(barrier, inc=1, device_id=dev, device_id_type=MESH)
        hello() if cond is None else pl.when(cond)(hello)

    g = jnp.broadcast_to(gain[...], (8, rows)).T[:, :1]
    base = pl.multiple_of(f * rows, rows)
    loads[0].wait()
    gate_o[pl.ds(base, rows), :] = (gw[...] * g).astype(jnp.bfloat16)
    loads[1].wait()
    dcol[f] = dw[...].astype(jnp.bfloat16)
    inner = jnp.logical_and(z > 0, z < n_z - 1)
    pl.when(inner)(lambda: pl.semaphore_wait(barrier, len(peers)))
    pl.when(jnp.logical_not(inner))(lambda: pl.semaphore_wait(barrier, len(peers) - 1))

    def lift():
        loads[2].wait()
        up_o[pl.ds(base, rows), :] = (uw[...] * g).astype(jnp.bfloat16)

    def norm():
        loads[3].wait()

        @pl.loop(0, n_tok // 64)
        def _(i):
            r = pl.multiple_of(i * 64, 64)
            v = tok[pl.ds(r, 64), :].astype(jnp.float32)
            v = v * lax.rsqrt(jnp.mean(v * v, axis=-1, keepdims=True) + eps_norm)
            v = v.astype(jnp.bfloat16)
            for j in range(n_z):
                normed[j, pl.ds(r, 64), :] = v[:, j * k_z : (j + 1) * k_z]

    def multiply(w, acc, src, first):
        zz = z_of(src)
        k0 = pl.multiple_of(zz * k_z, k_z)

        @pl.loop(0, n_tok // m_tile)
        def _(i):
            r = pl.multiple_of(i * m_tile, m_tile)
            a = normed[zz, pl.ds(r, m_tile), :]
            for c, n in col_tiles:
                v = jnp.dot(a, w[pl.ds(k0, k_z), c : c + n], preferred_element_type=jnp.float32)
                if first:
                    acc[pl.ds(r, m_tile), c : c + n] = v
                else:
                    acc[pl.ds(r, m_tile), c : c + n] += v

    def act():
        @pl.loop(0, n_tok // 32)
        def _(i):
            r = pl.multiple_of(i * 32, 32)
            v = acc_g[pl.ds(r, 32), :]
            hidden[pl.ds(r, 32), :] = (v / (1.0 + jnp.exp(-v)) * acc_u[pl.ds(r, 32), :]).astype(jnp.bfloat16)

    def arrived(c, q, n, lane):
        ref = down_o.at[:, pl.ds(pl.multiple_of(c * d_cols + q * part, part), n * part)]
        pltpu.make_async_remote_copy(
            ref, ref, link_send.at[0, 0], aa_recv.at[lane], device_id=(f, near), device_id_type=MESH,
        ).wait_recv()

    def product(c, q, n, out):
        @pl.loop(0, n_tok // m_tile)
        def _(i):
            r = pl.multiple_of(i * m_tile, m_tile)
            col = pl.multiple_of(c * d_cols + q * part, part)
            v = jnp.dot(
                hidden[pl.ds(r, m_tile), :], down_o[:, pl.ds(col, n * part)], preferred_element_type=jnp.float32
            )
            out[pl.ds(r, m_tile), :] = v.astype(jnp.bfloat16)

    def cols(q, n):
        return slice(q * part, (q + n) * part)

    def far_pair(i):
        q, n = FAR_GROUPS[i]
        return pltpu.make_async_remote_copy(
            far_a.at[:, cols(q, n)], far_in.at[:, cols(q, n)], fp_send.at[i], fp_recv.at[i],
            device_id=(f, near), device_id_type=MESH,
        )

    def across(i):
        q, n = FAR_GROUPS[i]
        return pltpu.make_async_remote_copy(
            out_send.at[:, cols(q, n)], out_in.at[:, cols(q, n)], ac_send.at[i], ac_recv.at[i],
            device_id=(f, far), device_id_type=MESH,
        )

    def hidden_copy():
        return pltpu.make_async_remote_copy(
            hidden, hidden_near, hid_send, hid_recv, device_id=(f, near), device_id_type=MESH,
        )

    def far_step(i):
        q, n = FAR_GROUPS[i]
        arrived(far_near, q, n, len(FAR_GROUPS) + i)
        product(far_near, q, n, far_a.at[:, cols(q, n)])
        far_pair(i).start()
        arrived(far, q, n, i)
        product(far, q, n, far_b.at[:, cols(q, n)])
        far_pair(i).wait_recv()
        out_send[:, cols(q, n)] = (
            far_b[:, cols(q, n)].astype(jnp.float32) + far_in[:, cols(q, n)].astype(jnp.float32)
        ).astype(jnp.bfloat16)
        across(i).start()

    def near_step(i):
        q, n = NEAR_GROUPS[i]
        col = pl.multiple_of(t * d_cols + q * part, part)
        for k in range(per):
            down_o[k * d_rows : (k + 1) * d_rows, pl.ds(col, n * part)] = dcol[t * per + k, :, cols(q, n)]

    def end():
        arrived(near, 0, 4, 2 * len(FAR_GROUPS))
        for i in range(len(FAR_GROUPS)):
            across(i).wait_recv()
        hidden_copy().wait_recv()

    done = {"gate": 0, "up": 0}
    for step in steps:
        play(step)
        what, i = step
        if what == "lift":
            lift()
        elif what == "norm":
            norm()
        elif what == "act":
            act()
            hidden_copy().start()
        elif what == "far":
            far_step(i)
        elif what == "near":
            near_step(i)
        elif what == "end":
            end()
        else:
            src = sources[0, what, i]
            for m in range(1, n_z):
                src = jnp.where(place == m, sources[m, what, i], src)
            multiply(gate_o if what == "gate" else up_o, acc_g if what == "gate" else acc_u, src, done[what] == 0)
            done[what] += 1

    for i in range(len(FAR_GROUPS)):
        far_pair(i).wait_send()
        across(i).wait_send()
    hidden_copy().wait_send()
    for m in range(n_z):
        @pl.when(place == m)
        def _(m=m):
            for what in WAYS:
                count = len(items[m, what])
                for i in range(max(0, count - RING), count):
                    transfer(m, what, i).wait_send()
            for step in steps:
                for what, item in before[m, step]:
                    if what == "core":
                        pl.when(elsewhere(item))(lambda item=item: to_core(item).wait_send())


def finish(
    n_tp, gate_i, up_i, down_i, dcol, hidden, hidden_near, out_in, gate_o, up_o, down_o, mix_o, near_w, mix, sems,
):
    t = lax.axis_index("tp")
    near = t + 1 - 2 * (t % 2)
    per = dcol.shape[0] // n_tp
    d_rows, d_cols = dcol.shape[1:]
    n_tok = hidden.shape[0]
    m_tile = min(256, n_tok)
    copies = [
        pltpu.make_async_copy(src, dst, sems.at[i])
        for i, (src, dst) in enumerate(((gate_i, gate_o), (up_i, up_o), (down_i, down_o), (mix, mix_o)))
    ]
    for copy in copies[:3]:
        copy.start()
    for k in range(per):
        near_w[k * d_rows : (k + 1) * d_rows, :] = dcol[near * per + k]
    col = pl.multiple_of(t * d_cols, d_cols)

    @pl.loop(0, n_tok // m_tile)
    def _(i):
        r = pl.ds(pl.multiple_of(i * m_tile, m_tile), m_tile)
        own = jnp.dot(hidden[r, :], down_i[:, pl.ds(col, d_cols)], preferred_element_type=jnp.float32)
        other = jnp.dot(hidden_near[r, :], near_w[...], preferred_element_type=jnp.float32)
        own, other = own.astype(jnp.bfloat16).astype(jnp.float32), other.astype(jnp.bfloat16).astype(jnp.float32)
        mix[r, :] = (own + other + out_in[r, :].astype(jnp.float32)).astype(jnp.bfloat16)

    copies[3].start()
    for copy in copies:
        copy.wait()


def line_on_device(n_fs, n_tp, tokens, norm_gain, gate_weight, up_weight, down_weight):
    n_tok, d_model = tokens.shape
    rows, width = gate_weight.shape
    d_rows, d_cols = down_weight.shape
    n_z = n_fs // 2
    n_p = len(PARTS)
    bf = jnp.bfloat16
    vmem = pl.BlockSpec(memory_space=pltpu.VMEM)
    dma = pltpu.SemaphoreType.DMA
    n_far = len(FAR_GROUPS)
    hbm = pl.BlockSpec(memory_space=pl.ANY)
    d_own = d_rows * n_fs // n_tp
    shapes = (
        (d_model, width), (d_model, width), (d_own, d_model), (n_fs, d_rows, d_cols),
        (n_tok, width), (n_tok, width), (n_tok, d_cols),
    )
    held = pl.pallas_call(
        functools.partial(line_kernel, n_fs, n_tp),
        out_shape=tuple(pltpu.VMEM(shape, bf) for shape in shapes),
        in_specs=[hbm, vmem, hbm, hbm, hbm],
        out_specs=(vmem,) * len(shapes),
        scratch_shapes=[
            pltpu.VMEM((n_tok, d_model), bf),
            pltpu.VMEM((rows, width), jnp.float32),
            pltpu.VMEM((rows, width), jnp.float32),
            pltpu.VMEM((d_rows, d_cols), jnp.float32),
            pltpu.VMEM((n_z, n_tok, d_model // n_z), bf),
            pltpu.VMEM((n_tok, width), jnp.float32),
            pltpu.VMEM((n_tok, width), jnp.float32),
            *[pltpu.VMEM((n_tok, d_cols), bf)] * 4,
            dma((4,)),
            dma((len(WAYS), RING)),
            dma((2 * len(DOWN),)),
            dma((n_fs, n_p)),
            dma((2 * n_far + 1,)),
            dma((n_far,)),
            dma((n_far,)),
            dma((n_far,)),
            dma((n_far,)),
            dma,
            dma,
        ],
        compiler_params=pltpu.CompilerParams(
            collective_id=0, has_side_effects=True, vmem_limit_bytes=30 * 2**20
        ),
    )(tokens, norm_gain[None, :], gate_weight, up_weight, down_weight)
    return pl.pallas_call(
        functools.partial(finish, n_tp),
        out_shape=tuple(
            jax.ShapeDtypeStruct(shape, bf)
            for shape in ((d_model, width), (d_model, width), (d_own, d_model), (n_tok, d_cols))
        ),
        in_specs=[vmem] * len(shapes),
        out_specs=(hbm,) * 4,
        scratch_shapes=[pltpu.VMEM((d_own, d_cols), bf), pltpu.VMEM((n_tok, d_cols), bf), dma((4,))],
        compiler_params=pltpu.CompilerParams(vmem_limit_bytes=6 * 2**20),
    )(*held)


def solution(mesh):
    n_fs, n_tp = mesh.shape["fs"], mesh.shape["tp"]
    in_specs = (P("fs", None), P("fs"), P("fs", "tp"), P("fs", "tp"), P("fs", "tp"))
    out_specs = (P(None, "tp"), P(None, "tp"), P("tp", None), P("fs", "tp"))
    body = line_on_device if (n_fs, n_tp) == (8, 4) else on_device
    return jax.shard_map(
        functools.partial(body, n_fs, n_tp), mesh=mesh, in_specs=in_specs, out_specs=out_specs, check_vma=False
    )
```

```python
import functools
import heapq

import jax
import jax.numpy as jnp
from jax import lax
from jax.experimental import pallas as pl
from jax.experimental.pallas import tpu as pltpu
from jax.sharding import PartitionSpec as P

eps_norm = 1e-06
MESH = pl.DeviceIdType.MESH

PIECES = (
    ("gate", 0, 1, "a"),
    ("gate", 1, 1, "a"),
    ("down", 2, 2, "b"),
    ("up", 0, 1, "a"),
    ("up", 1, 1, "a"),
    ("down", 0, 1, "a"),
    ("down", 1, 1, "a"),
)
PHASES = ((0, 1, 6), (2,), (3, 4), (5,))
GROUPS = ((1, 3, (2, 6)), (0, 1, (5,)))


def cost(p):
    return 0.5 if PIECES[p][0] == "down" and kind(p) == 1 else 1.0


def kind(p):
    return PIECES[p][3]


def plan(n_z):
    events = []
    seq = [(d, p) for phase in PHASES for d in range(1, n_z) for p in phase]
    order = sorted(range(len(PIECES)), key=lambda p: kind(p) == "a")
    own, total = {}, 0.0
    for p in order:
        total += cost(p)
        own[p] = total
    z_time, now = {}, 0.0
    for i, phase in enumerate(PHASES):
        for d in range(1, n_z):
            if d == n_z - 1 and i + 1 < len(PHASES):
                events.append((now + 0.02, 1, "launch", i + 1, 0))
            for p in phase:
                if kind(p) == "a":
                    now += cost(p)
                    z_time[d, p] = now
                    events.append((now, 0, "line", d, p))
                else:
                    now += 2.0 * cost(p)
                    z_time[d, p] = now
                    events.append((now - cost(p), 0, "line", d, p))
                    events.append((now, 0, "line_other", d, p))
    y_time = {}
    for z in range(n_z):
        at = total
        for d, p in seq:
            if kind(p) == "a":
                for zz in (z - d, z + d):
                    if 0 <= zz < n_z:
                        at = max(at, z_time[d, p]) + cost(p)
                        y_time[d, p] = max(y_time.get((d, p), 0.0), at)
    for p, at in own.items():
        events.append((at, 1, "pair", 0, p))
    for (d, p), at in y_time.items():
        events.append((at, 1, "pair", d, p))
    here = dict(y_time)
    here.update({(0, p): at for p, at in own.items()})
    last = 0.0
    for name in ("gate", "up"):
        mine = [p for p in range(len(PIECES)) if PIECES[p][0] == name]
        for d in range(n_z):
            at = max(here[d, p] for p in mine) + 0.01
            events.append((at, 2, "mul_" + name, d, 0))
            last = max(last, at)
    events.append((last + 0.01, 3, "act", 0, 0))
    end = max(e[0] for e in events) + 0.1
    for step in range(4):
        events.append((end + 0.01 + 0.01 * step, 4, "share", 0, step))
    for step in range(5):
        events.append((end + 0.1 + 0.1 * step, 4, "share", 1, step))
    events.append((end + 0.35, 4, "share", 0, 4))
    return sorted(events)


def kernel(
    n_fs, n_tp, tok_hbm, gain, gw, uw, dw, gate_o, up_o, down_o, mix_o,
    tok, dcol, normed, acc_g, acc_u, hidden, share0, share1, pair0, pair1, send0, send1, in0, in1,
    tok_sem, ag_send, ag_recv, aa_send, aa_recv, rs_send, rs_recv,
):
    tok_copy = pltpu.make_async_copy(tok_hbm, tok, tok_sem)
    tok_copy.start()
    shares, pairs, sends, ins = (share0, share1), (pair0, pair1), (send0, send1), (in0, in1)
    f, t = lax.axis_index("fs"), lax.axis_index("tp")
    n_z = n_fs // 2
    z, y = f // 2, f % 2
    per = n_fs // n_tp
    rows = gw.shape[0]
    d_rows, d_cols = dw.shape
    part = d_cols // 4
    n_tok = tok.shape[0]
    k_z = normed.shape[2]
    m_tile = min(256, n_tok)
    width = gw.shape[1]
    col_tiles = [(c, min(512, width - c)) for c in range(0, width, 512)]

    def flip(bit):
        return t + bit - 2 * bit * ((t // bit) % 2)

    near, far = flip(1), flip(2)
    far_near = far + 1 - 2 * (far % 2)

    def view(o, p):
        name, h, n, _ = PIECES[p]
        if name == "down":
            return dcol.at[o, :, pl.ds(h * part, n * part)]
        ref = gate_o if name == "gate" else up_o
        return ref.at[pl.ds(pl.multiple_of(o * rows + h * (rows // 2), rows // 2), rows // 2), :]

    def ag(o, p, way, dest):
        v = view(o, p)
        return pltpu.make_async_remote_copy(
            v, v, ag_send.at[o, p, way], ag_recv.at[o, p],
            device_id=(dest, t), device_id_type=MESH,
        )

    started = []

    def start(cond, make):
        if cond is None:
            make().start()
        else:
            pl.when(cond)(lambda: make().start())
        started.append((cond, make))

    def land(o, p):
        ag(o, p, 0, f).wait_recv()

    def exchange(cond, o, p):
        name, h, n, _ = PIECES[p]
        if name != "down":
            return
        owner = o // per
        k = o % per
        row = pl.multiple_of(k * d_rows, d_rows)
        col = pl.multiple_of(t * d_cols + h * part, part)

        def make():
            return pltpu.make_async_remote_copy(
                view(o, p), down_o.at[pl.ds(row, d_rows), pl.ds(col, n * part)],
                aa_send.at[o, p], aa_recv.at[t, k, p],
                device_id=(f, owner), device_id_type=MESH,
            )

        away = owner != t
        start(away if cond is None else jnp.logical_and(cond, away), make)
        mine = owner == t

        @pl.when(mine if cond is None else jnp.logical_and(cond, mine))
        def _():
            down_o[pl.ds(row, d_rows), pl.ds(col, n * part)] = dcol[o, :, h * part : (h + n) * part]

    barrier = pltpu.get_barrier_semaphore()
    other_y = f + 1 - 2 * y
    peers = [
        (z > 0, (f - 2, t)), (z < n_z - 1, (f + 2, t)), (None, (other_y, t)),
        (None, (f, near)), (None, (f, far)), (None, (f, far_near)),
    ]
    for cond, dev in peers:
        def hello(dev=dev):
            pl.semaphore_signal(barrier, inc=1, device_id=dev, device_id_type=MESH)
        hello() if cond is None else pl.when(cond)(hello)

    g = jnp.broadcast_to(gain[...], (8, rows)).T[:, :1]
    base = pl.multiple_of(f * rows, rows)
    gate_o[pl.ds(base, rows), :] = (gw[...] * g).astype(jnp.bfloat16)
    dcol[f] = dw[...].astype(jnp.bfloat16)
    up_o[pl.ds(base, rows), :] = (uw[...] * g).astype(jnp.bfloat16)
    inner = jnp.logical_and(z > 0, z < n_z - 1)
    pl.when(inner)(lambda: pl.semaphore_wait(barrier, len(peers)))
    pl.when(jnp.logical_not(inner))(lambda: pl.semaphore_wait(barrier, len(peers) - 1))

    def launch(phase):
        for p in PHASES[phase]:
            start(z > 0, functools.partial(ag, f, p, 0, f - 2))
            start(z < n_z - 1, functools.partial(ag, f, p, 1, f + 2))
            if kind(p) == "b":
                other_b(p)

    def other_b(p):
        start(z > 0, functools.partial(ag, other_y, p, 0, f - 2))
        start(z < n_z - 1, functools.partial(ag, other_y, p, 1, f + 2))

    for p in sorted(range(len(PIECES)), key=lambda p: kind(p) == "a"):
        start(None, functools.partial(ag, f, p, 2, other_y))
    for p in PHASES[0]:
        start(z > 0, functools.partial(ag, f, p, 0, f - 2))
        start(z < n_z - 1, functools.partial(ag, f, p, 1, f + 2))
    for p in range(len(PIECES)):
        exchange(None, f, p)

    n_norm = n_tok // 64
    tok_copy.wait()

    @pl.loop(0, n_norm)
    def _(i):
        r = pl.multiple_of(i * 64, 64)
        x = tok[pl.ds(r, 64), :].astype(jnp.float32)
        x = x * lax.rsqrt(jnp.mean(x * x, axis=-1, keepdims=True) + eps_norm)
        x = x.astype(jnp.bfloat16)
        for j in range(n_z):
            normed[j, pl.ds(r, 64), :] = x[:, j * k_z : (j + 1) * k_z]

    def multiply(w, acc, zz, first):
        k0 = pl.multiple_of(zz * k_z, k_z)

        @pl.loop(0, n_tok // m_tile)
        def _(i):
            r = pl.multiple_of(i * m_tile, m_tile)
            a = normed[zz, pl.ds(r, m_tile), :]
            for c, n in col_tiles:
                v = jnp.dot(a, w[pl.ds(k0, k_z), c : c + n], preferred_element_type=jnp.float32)
                if first:
                    acc[pl.ds(r, m_tile), c : c + n] = v
                else:
                    acc[pl.ds(r, m_tile), c : c + n] += v

    def sides(d):
        return [(z >= d, z - d, -1), (z + d < n_z, z + d, 1)]

    def forward(cond, zz, sign, o, p):
        if sign < 0:
            start(jnp.logical_and(cond, z < n_z - 1), functools.partial(ag, o, p, 1, f + 2))
        else:
            start(jnp.logical_and(cond, z > 0), functools.partial(ag, o, p, 0, f - 2))

    def share_step(group, step):
        q, n, parts = GROUPS[group]
        share, half_in, out_send, out_in = shares[group], pairs[group], sends[group], ins[group]
        wide = n * part

        def aa_wait(c):
            for k in range(per):
                for p in parts:
                    _, h, m, _ = PIECES[p]
                    ref = down_o.at[
                        pl.ds(k * d_rows, d_rows), pl.ds(pl.multiple_of(c * d_cols + h * part, part), m * part)
                    ]
                    pltpu.make_async_remote_copy(
                        ref, ref, aa_send.at[0, p], aa_recv.at[c, k, p], device_id=(f, near), device_id_type=MESH,
                    ).wait_recv()

        def product(c, slot):
            @pl.loop(0, n_tok // m_tile)
            def _(i):
                r = pl.multiple_of(i * m_tile, m_tile)
                col = pl.multiple_of(c * d_cols + q * part, part)
                v = jnp.dot(hidden[pl.ds(r, m_tile), :], down_o[:, pl.ds(col, wide)], preferred_element_type=jnp.float32)
                share[slot, pl.ds(r, m_tile), :] = v.astype(jnp.bfloat16)

        def pair(slot):
            return pltpu.make_async_remote_copy(
                share.at[slot], half_in.at[slot], rs_send.at[group, slot], rs_recv.at[group, slot],
                device_id=(f, near), device_id_type=MESH,
            )

        def across():
            return pltpu.make_async_remote_copy(
                out_send, out_in, rs_send.at[group, 2], rs_recv.at[group, 2],
                device_id=(f, far), device_id_type=MESH,
            )

        if step == 0:
            aa_wait(far_near)
            product(far_near, 0)
            start(None, functools.partial(pair, 0))
        elif step == 1:
            aa_wait(far)
            product(far, 2)
            pair(0).wait_recv()
            out_send[...] = (share[2].astype(jnp.float32) + half_in[0].astype(jnp.float32)).astype(jnp.bfloat16)
            start(None, across)
        elif step == 2:
            aa_wait(near)
            product(near, 1)
            start(None, functools.partial(pair, 1))
        elif step == 3:
            product(t, 3)
        elif step == 4:
            pair(1).wait_recv()
            across().wait_recv()
            mix_o[:, q * part : (q + n) * part] = (
                share[3].astype(jnp.float32) + half_in[1].astype(jnp.float32) + out_in[...].astype(jnp.float32)
            ).astype(jnp.bfloat16)

    for _, _, what, d, p in plan(n_z):
        if what == "launch":
            launch(d)
        elif what == "share":
            share_step(d, p)
        elif what == "line":
            for cond, zz, sign in sides(d):
                o = zz * 2 + y
                pl.when(cond)(functools.partial(land, o, p))
                forward(cond, zz, sign, o, p)
                if kind(p) == "a":
                    start(cond, functools.partial(ag, o, p, 2, other_y))
                exchange(cond, o, p)
        elif what == "line_other":
            for cond, zz, sign in sides(d):
                o = zz * 2 + 1 - y
                pl.when(cond)(functools.partial(land, o, p))
                forward(cond, zz, sign, o, p)
                exchange(cond, o, p)
        elif what == "pair":
            if d == 0:
                land(other_y, p)
                exchange(None, other_y, p)
            else:
                for cond, zz, sign in sides(d):
                    o = zz * 2 + 1 - y
                    pl.when(cond)(functools.partial(land, o, p))
                    exchange(cond, o, p)
        elif what == "mul_gate" or what == "mul_up":
            w, acc = (gate_o, acc_g) if what == "mul_gate" else (up_o, acc_u)
            if d == 0:
                multiply(w, acc, z, True)
            else:
                for cond, zz, sign in sides(d):
                    pl.when(cond)(functools.partial(multiply, w, acc, zz, False))
        elif what == "act":
            @pl.loop(0, n_tok // 32)
            def _(i):
                r = pl.multiple_of(i * 32, 32)
                v = acc_g[pl.ds(r, 32), :]
                hidden[pl.ds(r, 32), :] = (v / (1.0 + jnp.exp(-v)) * acc_u[pl.ds(r, 32), :]).astype(jnp.bfloat16)

    for cond, make in started:
        if cond is None:
            make().wait_send()
        else:
            pl.when(cond)(lambda make=make: make().wait_send())


def on_device(n_fs, n_tp, tokens, norm_gain, gate_weight, up_weight, down_weight):
    n_tok, d_model = tokens.shape
    rows, width = gate_weight.shape
    d_rows, d_cols = down_weight.shape
    part = d_cols // 4
    n_z = n_fs // 2
    n_p = len(PIECES)
    bf = jnp.bfloat16
    vmem = pl.BlockSpec(memory_space=pltpu.VMEM)
    dma = pltpu.SemaphoreType.DMA
    return pl.pallas_call(
        functools.partial(kernel, n_fs, n_tp),
        out_shape=(
            pltpu.VMEM((d_model, width), bf),
            pltpu.VMEM((d_model, width), bf),
            pltpu.VMEM((d_rows * n_fs // n_tp, d_model), bf),
            pltpu.VMEM((n_tok, d_cols), bf),
        ),
        in_specs=[pl.BlockSpec(memory_space=pl.ANY)] + [vmem] * 4,
        out_specs=(vmem,) * 4,
        scratch_shapes=[
            pltpu.VMEM((n_tok, d_model), bf),
            pltpu.VMEM((n_fs, d_rows, d_cols), bf),
            pltpu.VMEM((n_z, n_tok, d_model // n_z), bf),
            pltpu.VMEM((n_tok, width), jnp.float32),
            pltpu.VMEM((n_tok, width), jnp.float32),
            pltpu.VMEM((n_tok, width), bf),
            *[pltpu.VMEM((4, n_tok, g[1] * part), bf) for g in GROUPS],
            *[pltpu.VMEM((2, n_tok, g[1] * part), bf) for g in GROUPS],
            *[pltpu.VMEM((n_tok, g[1] * part), bf) for g in GROUPS],
            *[pltpu.VMEM((n_tok, g[1] * part), bf) for g in GROUPS],
            dma,
            dma((n_fs, n_p, 3)),
            dma((n_fs, n_p)),
            dma((n_fs, n_p)),
            dma((n_tp, n_fs // n_tp, n_p)),
            dma((2, 3)),
            dma((2, 3)),
        ],
        compiler_params=pltpu.CompilerParams(
            collective_id=0, has_side_effects=True, vmem_limit_bytes=46 * 2**20
        ),
    )(tokens, norm_gain[None, :], gate_weight, up_weight, down_weight)


PARTS = (
    ("gate", 0, 8),
    ("gate", 8, 8),
    ("up", 0, 8),
    ("up", 8, 4),
    ("up", 12, 4),
    ("down", 0, 1),
    ("down", 1, 1),
    ("down", 2, 1),
    ("down", 3, 1),
)
REACH = (
    ((0, 2), (0, 2), (0, 1), (0, 3), (0, 1), (0, 0), (0, 0), (0, 0), (0, 0)),
    ((1, 1), (1, 3), (1, 1), (1, 1), (1, 1), (1, 1), (0, 3), (0, 1), (1, 1)),
    ((2, 2), (2, 2), (2, 2), (2, 2), (2, 2), (2, 3), (0, 3), (2, 2), (2, 2)),
    ((2, 3), (2, 3), (0, 3), (3, 3), (2, 3), (3, 3), (0, 3), (3, 3), (1, 3)),
)
RANKS = (
    (0.98, 2.75, 3.09, 4.72, 2.28, 7.34, 5.35, 5.05, 5.57),
    (-0.59, 0.97, 3.70, 3.76, 0.58, 8.74, 11.15, 6.05, 10.14),
    (2.58, 3.18, 1.14, 4.50, 1.86, 1.38, 1.00, 0.63, 2.20),
    (4.44, 4.79, 5.54, 4.72, 3.65, 0.90, 4.97, 3.57, 3.69),
)
CROSS = (
    (1.79, 1.76, 1.17, 0.05, -0.15, 1.84, 1.49, 3.23, 0.29),
    (1.91, 0.67, 1.91, 2.54, 2.95, 0.66, 1.52, 0.56, 2.95),
    (-0.24, 2.08, 0.64, 2.98, 3.67, -0.32, 1.30, -0.30, 0.21),
    (0.46, 0.19, 3.29, 3.55, 2.08, 2.08, 1.84, 1.78, -0.37),
)
OTHER_SIDE = -0.3
DOWN = tuple(p for p in range(len(PARTS)) if PARTS[p][0] == "down")
FAR_GROUPS = ((0, 2), (2, 2))
NEAR_GROUPS = ((0, 2), (2, 1), (3, 1))
UNIT, LAG, LEAD = 7.73, 2.0, 10.0
WAYS = ("up", "dn", "y", "x")
RING = 6


def crossing(src, p, n_z):
    return PARTS[p][0] == "down" and 2 * src >= n_z


def length(p):
    return UNIT * (0.5 if PARTS[p][0] == "down" else PARTS[p][2] / 8)


def rank(m, link, item):
    src, side, p = item
    if link == "y" and REACH[src][p] != (src, src):
        return CROSS[src][p]
    return RANKS[src][p] + OTHER_SIDE * side + 0.01 * abs(src - m)


def simulate(n_z):
    queue, free, sent = {}, {}, {}
    events, have = [], [{} for _ in range(n_z)]
    far_in = [{} for _ in range(n_z)]
    count = [0]
    for m in range(n_z):
        for link in ("up", "dn", "y", "x"):
            queue[m, link], free[m, link], sent[m, link] = [], True, []

    def add(at, what, *rest):
        count[0] += 1
        heapq.heappush(events, (at, count[0], what, rest))

    def kick(at, m, link):
        if free[m, link] and queue[m, link]:
            queue[m, link].sort()
            _, item = queue[m, link].pop(0)
            free[m, link] = False
            sent[m, link].append((at, item))
            add(at + length(item[2]), "free", m, link)
            add(at + length(item[2]) + LAG, "land", m, link, item)

    def put(at, m, link, item):
        queue[m, link].append((rank(m, link, item), item))
        kick(at, m, link)

    def got(at, m, item):
        src, side, p = item
        have[m][item] = at
        low, high = REACH[src][p]
        if m >= src and m < (n_z - 1 if side == 0 else high):
            put(at, m, "up", item)
        if m <= src and m > (0 if side == 0 else low):
            put(at, m, "dn", item)
        if side == 0 and (m == src or not low <= m <= high):
            put(at, m, "y", item)
        if crossing(src, p, n_z):
            put(at, m, "x", item)

    for m in range(n_z):
        for p in range(len(PARTS)):
            add(1.0 if PARTS[p][0] == "up" else 0.0, "own", m, (m, 0, p))
    while events:
        at, _, what, rest = heapq.heappop(events)
        if what == "own":
            got(at, *rest)
        elif what == "free":
            free[rest] = True
            kick(at, *rest)
        else:
            m, link, item = rest
            if link == "x":
                far_in[n_z - 1 - m][item] = at
            elif link == "y":
                got(at, m, (item[0], 1, item[2]))
            else:
                got(at, m + (1 if link == "up" else -1), item)
    return have, far_in, sent


def timetable(n_z):
    have, far_in, sent = simulate(n_z)
    sources, ready = {}, {}
    for m in range(n_z):
        for name in ("gate", "up"):
            mine = [p for p in range(len(PARTS)) if PARTS[p][0] == name]
            done = sorted((max(have[m][src, side, p] for side in (0, 1) for p in mine), src) for src in range(n_z))
            for j, (at, src) in enumerate(done):
                sources[m, name, j], ready[m, (name, j)] = src, at
        ready[m, ("lift", 0)] = 0.5
        ready[m, ("norm", 0)] = 1.5
        ready[m, ("act", 0)] = 0.0
        for g, (q, n) in enumerate(FAR_GROUPS):
            ready[m, ("far", g)] = max(at for item, at in far_in[m].items() if q <= PARTS[item[2]][1] < q + n)
        for g, (q, n) in enumerate(NEAR_GROUPS):
            ready[m, ("near", g)] = max(
                at for item, at in have[m].items()
                if PARTS[item[2]][0] == "down" and not crossing(item[0], item[2], n_z) and q <= PARTS[item[2]][1] < q + n
            )
        ready[m, ("end", 0)] = 1e9
    muls = sorted(
        (sum(ready[m, (name, j)] for m in range(n_z)), name, j) for name in ("gate", "up") for j in range(n_z)
    )
    steps = [("lift", 0), ("norm", 0)] + [(name, j) for _, name, j in muls] + [("act", 0)]
    steps += [("far", g) for g in range(len(FAR_GROUPS))] + [("near", g) for g in range(len(NEAR_GROUPS))] + [("end", 0)]
    spans = {"lift": 0.5, "norm": 3.0, "gate": 1.5, "up": 1.5, "act": 1.5, "far": 3.0, "near": 0.2, "end": 0.0}
    before = {}
    for m in range(n_z):
        todo = [(at, 0, "wait", item) for item, at in have[m].items() if item[:2] != (m, 0)]
        for link in WAYS:
            last = 0.0
            for i, (at, item) in enumerate(sent[m, link]):
                last = max(last, have[m][item], at - LEAD)
                todo.append((last, 1, link, i))
        for item, at in have[m].items():
            if PARTS[item[2]][0] == "down" and not crossing(item[0], item[2], n_z):
                todo.append((at, 1, "core", item))
        todo.sort(key=lambda e: e[:2])
        now = 0.0
        for step in steps:
            now = max(now, ready[m, step])
            before[m, step] = [e[2:] for e in todo if e[0] <= now]
            todo = [e for e in todo if e[0] > now]
            now += spans[step[0]]
    items = {key: [item for _, item in log] for key, log in sent.items()}
    return steps, sources, before, items


def line_kernel(
    n_fs, n_tp, tok_hbm, gain, gw_hbm, uw_hbm, dw_hbm, gate_o, up_o, down_o, dcol, hidden, hidden_near, out_in,
    tok, gw, uw, dw, normed, acc_g, acc_u, far_a, far_b, far_in, out_send,
    in_sem, link_send, core_send, ag_recv, aa_recv, fp_send, fp_recv, ac_send, ac_recv, hid_send, hid_recv,
):
    loads = [
        pltpu.make_async_copy(src, dst, in_sem.at[i])
        for i, (src, dst) in enumerate(((gw_hbm, gw), (dw_hbm, dw), (uw_hbm, uw), (tok_hbm, tok)))
    ]
    for load in loads:
        load.start()
    f, t = lax.axis_index("fs"), lax.axis_index("tp")
    n_z = n_fs // 2
    z, y = f // 2, f % 2
    x = t // 2
    per = n_fs // n_tp
    rows = gw.shape[0]
    d_rows, d_cols = dw.shape
    part = d_cols // 4
    n_tok = tok.shape[0]
    k_z = normed.shape[2]
    m_tile = min(256, n_tok)
    width = gw.shape[1]
    col_tiles = [(c, min(512, width - c)) for c in range(0, width, 512)]
    place = z + x * (n_z - 1 - 2 * z)
    ahead = f + 2 - 4 * x
    behind = f - 2 + 4 * x
    other_y = f + 1 - 2 * y
    near = t + 1 - 2 * (t % 2)
    far = t + 2 - 4 * x
    far_near = far + 1 - 2 * (far % 2)
    steps, sources, before, items = timetable(n_z)

    def z_of(src):
        return src + x * (n_z - 1 - 2 * src)

    def owner_of(item):
        src, side, _ = item
        return 2 * z_of(src) + (y if side == 0 else 1 - y)

    def view(o, p):
        name, first, n = PARTS[p]
        if name == "down":
            return dcol.at[o, first]
        ref = gate_o if name == "gate" else up_o
        step = rows // 16
        return ref.at[pl.ds(pl.multiple_of(o * rows + first * step, step), n * step), :]

    def ag(item, send, dest):
        o, p = owner_of(item), item[2]
        v = view(o, p)
        return pltpu.make_async_remote_copy(
            v, v, send, ag_recv.at[o, p], device_id=(dest, t), device_id_type=MESH,
        )

    def hand(item, send):
        o, p = owner_of(item), item[2]
        _, first, n = PARTS[p]
        group = [q <= first < q + m for q, m in FAR_GROUPS].index(True)
        lane = (t + o // per) % 2 * len(FAR_GROUPS) + group if crossing(item[0], p, n_z) else 2 * len(FAR_GROUPS)
        row = pl.multiple_of((o % per) * d_rows, d_rows)
        col = pl.multiple_of(t * d_cols + first * part, part)
        return pltpu.make_async_remote_copy(
            view(o, p), down_o.at[pl.ds(row, d_rows), pl.ds(col, n * part)],
            send, aa_recv.at[lane], device_id=(f, o // per), device_id_type=MESH,
        )

    def transfer(m, what, i):
        item, send = items[m, what][i], link_send.at[WAYS.index(what), i % RING]
        if what == "x":
            return hand(item, send)
        return ag(item, send, {"up": ahead, "dn": behind, "y": other_y}[what])

    def to_core(item):
        return hand(item, core_send.at[item[1] * len(DOWN) + DOWN.index(item[2])])

    def elsewhere(item):
        return owner_of(item) // per != t

    def play(step):
        for m in range(n_z):
            def events(m=m):
                for what, item in before[m, step]:
                    if what == "wait":
                        ag(item, link_send.at[0, 0], f).wait_recv()
                    elif what == "core":
                        pl.when(elsewhere(item))(lambda item=item: to_core(item).start())
                    else:
                        if item >= RING:
                            transfer(m, what, item - RING).wait_send()
                        transfer(m, what, item).start()
            if before[m, step]:
                pl.when(place == m)(events)

    barrier = pltpu.get_barrier_semaphore()
    peers = [
        (z > 0, (f - 2, t)), (z < n_z - 1, (f + 2, t)), (None, (other_y, t)),
        (None, (f, near)), (None, (f, far)), (None, (f, far_near)),
    ]
    for cond, dev in peers:
        def hello(dev=dev):
            pl.semaphore_signal(barrier, inc=1, device_id=dev, device_id_type=MESH)
        hello() if cond is None else pl.when(cond)(hello)

    g = jnp.broadcast_to(gain[...], (8, rows)).T[:, :1]
    base = pl.multiple_of(f * rows, rows)
    loads[0].wait()
    gate_o[pl.ds(base, rows), :] = (gw[...] * g).astype(jnp.bfloat16)
    loads[1].wait()
    for j in range(4):
        dcol[f, j] = dw[:, j * part : (j + 1) * part].astype(jnp.bfloat16)
    inner = jnp.logical_and(z > 0, z < n_z - 1)
    pl.when(inner)(lambda: pl.semaphore_wait(barrier, len(peers)))
    pl.when(jnp.logical_not(inner))(lambda: pl.semaphore_wait(barrier, len(peers) - 1))

    def lift():
        loads[2].wait()
        up_o[pl.ds(base, rows), :] = (uw[...] * g).astype(jnp.bfloat16)

    def norm():
        loads[3].wait()

        @pl.loop(0, n_tok // 64)
        def _(i):
            r = pl.multiple_of(i * 64, 64)
            v = tok[pl.ds(r, 64), :].astype(jnp.float32)
            v = v * lax.rsqrt(jnp.mean(v * v, axis=-1, keepdims=True) + eps_norm)
            v = v.astype(jnp.bfloat16)
            for j in range(n_z):
                normed[j, pl.ds(r, 64), :] = v[:, j * k_z : (j + 1) * k_z]

    def multiply(w, acc, src, first):
        zz = z_of(src)
        k0 = pl.multiple_of(zz * k_z, k_z)

        @pl.loop(0, n_tok // m_tile)
        def _(i):
            r = pl.multiple_of(i * m_tile, m_tile)
            a = normed[zz, pl.ds(r, m_tile), :]
            for c, n in col_tiles:
                v = jnp.dot(a, w[pl.ds(k0, k_z), c : c + n], preferred_element_type=jnp.float32)
                if first:
                    acc[pl.ds(r, m_tile), c : c + n] = v
                else:
                    acc[pl.ds(r, m_tile), c : c + n] += v

    def act():
        @pl.loop(0, n_tok // 32)
        def _(i):
            r = pl.multiple_of(i * 32, 32)
            v = acc_g[pl.ds(r, 32), :]
            hidden[pl.ds(r, 32), :] = (v / (1.0 + jnp.exp(-v)) * acc_u[pl.ds(r, 32), :]).astype(jnp.bfloat16)

    def arrived(c, q, n, lane):
        ref = down_o.at[:, pl.ds(pl.multiple_of(c * d_cols + q * part, part), n * part)]
        pltpu.make_async_remote_copy(
            ref, ref, link_send.at[0, 0], aa_recv.at[lane], device_id=(f, near), device_id_type=MESH,
        ).wait_recv()

    def product(c, q, n, out):
        @pl.loop(0, n_tok // m_tile)
        def _(i):
            r = pl.multiple_of(i * m_tile, m_tile)
            col = pl.multiple_of(c * d_cols + q * part, part)
            v = jnp.dot(
                hidden[pl.ds(r, m_tile), :], down_o[:, pl.ds(col, n * part)], preferred_element_type=jnp.float32
            )
            out[pl.ds(r, m_tile), :] = v.astype(jnp.bfloat16)

    def cols(q, n):
        return slice(q * part, (q + n) * part)

    def far_pair(i):
        q, n = FAR_GROUPS[i]
        return pltpu.make_async_remote_copy(
            far_a.at[:, cols(q, n)], far_in.at[:, cols(q, n)], fp_send.at[i], fp_recv.at[i],
            device_id=(f, near), device_id_type=MESH,
        )

    def across(i):
        q, n = FAR_GROUPS[i]
        return pltpu.make_async_remote_copy(
            out_send.at[:, cols(q, n)], out_in.at[:, cols(q, n)], ac_send.at[i], ac_recv.at[i],
            device_id=(f, far), device_id_type=MESH,
        )

    def hidden_copy():
        return pltpu.make_async_remote_copy(
            hidden, hidden_near, hid_send, hid_recv, device_id=(f, near), device_id_type=MESH,
        )

    def far_step(i):
        q, n = FAR_GROUPS[i]
        arrived(far_near, q, n, len(FAR_GROUPS) + i)
        product(far_near, q, n, far_a.at[:, cols(q, n)])
        far_pair(i).start()
        arrived(far, q, n, i)
        product(far, q, n, far_b.at[:, cols(q, n)])
        far_pair(i).wait_recv()
        out_send[:, cols(q, n)] = (
            far_b[:, cols(q, n)].astype(jnp.float32) + far_in[:, cols(q, n)].astype(jnp.float32)
        ).astype(jnp.bfloat16)
        across(i).start()

    def near_step(i):
        q, n = NEAR_GROUPS[i]
        for j in range(q, q + n):
            col = pl.multiple_of(t * d_cols + j * part, part)
            for k in range(per):
                down_o[k * d_rows : (k + 1) * d_rows, pl.ds(col, part)] = dcol[t * per + k, j]

    def end():
        arrived(near, 0, 4, 2 * len(FAR_GROUPS))
        for i in range(len(FAR_GROUPS)):
            across(i).wait_recv()
        hidden_copy().wait_recv()

    done = {"gate": 0, "up": 0}
    for step in steps:
        play(step)
        what, i = step
        if what == "lift":
            lift()
        elif what == "norm":
            norm()
        elif what == "act":
            act()
            hidden_copy().start()
        elif what == "far":
            far_step(i)
        elif what == "near":
            near_step(i)
        elif what == "end":
            end()
        else:
            src = sources[0, what, i]
            for m in range(1, n_z):
                src = jnp.where(place == m, sources[m, what, i], src)
            multiply(gate_o if what == "gate" else up_o, acc_g if what == "gate" else acc_u, src, done[what] == 0)
            done[what] += 1

    for i in range(len(FAR_GROUPS)):
        far_pair(i).wait_send()
        across(i).wait_send()
    hidden_copy().wait_send()
    for m in range(n_z):
        @pl.when(place == m)
        def _(m=m):
            for what in WAYS:
                count = len(items[m, what])
                for i in range(max(0, count - RING), count):
                    transfer(m, what, i).wait_send()
            for step in steps:
                for what, item in before[m, step]:
                    if what == "core":
                        pl.when(elsewhere(item))(lambda item=item: to_core(item).wait_send())


def finish(
    n_tp, gate_i, up_i, down_i, dcol, hidden, hidden_near, out_in, gate_o, up_o, down_o, mix_o, near_w, mix, sems,
):
    t = lax.axis_index("tp")
    near = t + 1 - 2 * (t % 2)
    per = dcol.shape[0] // n_tp
    parts, d_rows, part = dcol.shape[1:]
    d_cols = parts * part
    n_tok = hidden.shape[0]
    m_tile = min(256, n_tok)
    copies = [
        pltpu.make_async_copy(src, dst, sems.at[i])
        for i, (src, dst) in enumerate(((gate_i, gate_o), (up_i, up_o), (down_i, down_o), (mix, mix_o)))
    ]
    for copy in copies[:3]:
        copy.start()
    for k in range(per):
        for j in range(parts):
            near_w[k * d_rows : (k + 1) * d_rows, j * part : (j + 1) * part] = dcol[near * per + k, j]
    col = pl.multiple_of(t * d_cols, d_cols)

    @pl.loop(0, n_tok // m_tile)
    def _(i):
        r = pl.ds(pl.multiple_of(i * m_tile, m_tile), m_tile)
        own = jnp.dot(hidden[r, :], down_i[:, pl.ds(col, d_cols)], preferred_element_type=jnp.float32)
        other = jnp.dot(hidden_near[r, :], near_w[...], preferred_element_type=jnp.float32)
        own, other = own.astype(jnp.bfloat16).astype(jnp.float32), other.astype(jnp.bfloat16).astype(jnp.float32)
        mix[r, :] = (own + other + out_in[r, :].astype(jnp.float32)).astype(jnp.bfloat16)

    copies[3].start()
    for copy in copies:
        copy.wait()


def line_on_device(n_fs, n_tp, tokens, norm_gain, gate_weight, up_weight, down_weight):
    n_tok, d_model = tokens.shape
    rows, width = gate_weight.shape
    d_rows, d_cols = down_weight.shape
    n_z = n_fs // 2
    n_p = len(PARTS)
    bf = jnp.bfloat16
    vmem = pl.BlockSpec(memory_space=pltpu.VMEM)
    dma = pltpu.SemaphoreType.DMA
    n_far = len(FAR_GROUPS)
    hbm = pl.BlockSpec(memory_space=pl.ANY)
    d_own = d_rows * n_fs // n_tp
    shapes = (
        (d_model, width), (d_model, width), (d_own, d_model), (n_fs, 4, d_rows, d_cols // 4),
        (n_tok, width), (n_tok, width), (n_tok, d_cols),
    )
    held = pl.pallas_call(
        functools.partial(line_kernel, n_fs, n_tp),
        out_shape=tuple(pltpu.VMEM(shape, bf) for shape in shapes),
        in_specs=[hbm, vmem, hbm, hbm, hbm],
        out_specs=(vmem,) * len(shapes),
        scratch_shapes=[
            pltpu.VMEM((n_tok, d_model), bf),
            pltpu.VMEM((rows, width), jnp.float32),
            pltpu.VMEM((rows, width), jnp.float32),
            pltpu.VMEM((d_rows, d_cols), jnp.float32),
            pltpu.VMEM((n_z, n_tok, d_model // n_z), bf),
            pltpu.VMEM((n_tok, width), jnp.float32),
            pltpu.VMEM((n_tok, width), jnp.float32),
            *[pltpu.VMEM((n_tok, d_cols), bf)] * 4,
            dma((4,)),
            dma((len(WAYS), RING)),
            dma((2 * len(DOWN),)),
            dma((n_fs, n_p)),
            dma((2 * n_far + 1,)),
            dma((n_far,)),
            dma((n_far,)),
            dma((n_far,)),
            dma((n_far,)),
            dma,
            dma,
        ],
        compiler_params=pltpu.CompilerParams(
            collective_id=0, has_side_effects=True, vmem_limit_bytes=30 * 2**20
        ),
    )(tokens, norm_gain[None, :], gate_weight, up_weight, down_weight)
    return pl.pallas_call(
        functools.partial(finish, n_tp),
        out_shape=tuple(
            jax.ShapeDtypeStruct(shape, bf)
            for shape in ((d_model, width), (d_model, width), (d_own, d_model), (n_tok, d_cols))
        ),
        in_specs=[vmem] * len(shapes),
        out_specs=(hbm,) * 4,
        scratch_shapes=[pltpu.VMEM((d_own, d_cols), bf), pltpu.VMEM((n_tok, d_cols), bf), dma((4,))],
        compiler_params=pltpu.CompilerParams(vmem_limit_bytes=6 * 2**20),
    )(*held)


def solution(mesh):
    n_fs, n_tp = mesh.shape["fs"], mesh.shape["tp"]
    in_specs = (P("fs", None), P("fs"), P("fs", "tp"), P("fs", "tp"), P("fs", "tp"))
    out_specs = (P(None, "tp"), P(None, "tp"), P("tp", None), P("fs", "tp"))
    body = line_on_device if (n_fs, n_tp) == (8, 4) else on_device
    return jax.shard_map(
        functools.partial(body, n_fs, n_tp), mesh=mesh, in_specs=in_specs, out_specs=out_specs, check_vma=False
    )
```
